32 devices in a mesh: ep: 8 (over z, y), tp: 4 (over x, core).
Axes of the slice: x: 2, y: 2, z: 4, core: 2. Of those that a mesh axis runs over, the one named last changes fastest.
Arguments:
- tokens: bfloat16 [1024, 2048], P('ep'), may hold values from -6 to 6
- norm_gain: float32 [2048], replicated, may hold values from 0.1 to 1.9
- routes: int32 [1024, 2], P('ep'), may hold values from 0 to 7, all different within a row; in each aligned block of 128 rows (0 to 127, 128 to 255, ...) at most 48 rows name the same one
- group_prob: float32 [1024], P('ep'), may hold values from 0.2 to 1
- expert_logits: float32 [1024, 2], P('ep'), may hold values from -6 to 6
- gate_weight: bfloat16 [8, 2048, 384], P('ep', None, 'tp'), may hold values from -0.125 to 0.125
- up_weight: bfloat16 [8, 2048, 384], P('ep', None, 'tp'), may hold values from -0.125 to 0.125
- down_matrix: bfloat16 [8, 384, 2048], P('ep', 'tp'), may hold values from -0.3125 to 0.3125
Outputs:
- combined: bfloat16 [1024, 2048], P('ep', 'tp')
The draws below stay inside these ranges and needn't reach their ends.
Inputs may be any that keep to these rules, and one draw needn't show every extreme that they name: `routes`: each row names 2 different experts. Among the 128 tokens of one index of ep at most 48 rows name one expert, and in every draw some expert is named by exactly 48 of them.
All inputs are finite; a program needn't handle non-finite values.
Results may differ from the reference program's by a relative error of at most 0.013.
Values may be sent and summed in bfloat16 or wider, within the bound.
A program may use at most 64 MiB of HBM per device.

```python
import math
import jax
import jax.numpy as jnp
import numpy as np
from jax import lax

MODEL_DIM = 2048
FF = 384
TOPK = 2
TOK_DEV = 128
EXPERTS = 8
CAP = 48
TOKENS = 1024
N_EP = 8
N_TP = 4


def shard_levels(key, shape, split, least, high):
    level, own = 1.0, jax.random.fold_in(key, 6)
    for axis_at, shards_of in split:
        draws = jnp.exp(jax.random.uniform(jax.random.fold_in(own, axis_at), (shards_of,), jnp.float32, least / len(split), high / len(split)))
        level = level * jnp.repeat(draws, shape[axis_at] // shards_of).reshape([-1 if axis == axis_at else 1 for axis in range(len(shape))])
    return level


def assign_block(stream_key, own, number, rows, number_of, top, limit, lean):
    sequence = jax.random.permutation(stream_key, number_of)
    heavy_load, common = shares(number_of, rows * top, limit, lean, True), shares(number_of, rows * top, limit, lean, False)
    places = jnp.arange(number_of)

    def named(lengths, turn):
        used = int((lengths > 0).sum())
        fixed = max(1, used // 4)
        passed = fixed + (places - fixed + turn * (used - fixed)) % max(1, number_of - fixed)
        return jnp.zeros((number_of,), jnp.int32).at[sequence[jnp.where(places < fixed, places, passed)]].set(jnp.asarray(lengths, jnp.int32))

    lengths = jnp.where(number % 4 == 0, named(heavy_load, number // 4), named(common, number - number // 4 - 1))
    mixed = jax.random.permutation(jax.random.fold_in(own, 3), number_of)
    giver, receiver = mixed[0:number_of // 2 * 2:2], mixed[1:number_of // 2 * 2:2]
    room = jnp.minimum(lengths[giver] - 1, limit - lengths[receiver]) // 2
    room = jnp.where((giver == sequence[0]) | (receiver == sequence[0]) | (lengths[receiver] == 0), 0, jnp.maximum(room, 0))
    passed = jax.random.randint(jax.random.fold_in(own, 4), (number_of // 2,), 0, 1 << 20) % (room + 1)
    lengths = lengths.at[giver].add(-passed).at[receiver].add(passed)
    labels = jnp.searchsorted(jnp.cumsum(lengths), jnp.arange(rows * top), side="right").astype(jnp.int32)
    listing = labels.reshape(top, rows).T
    listing = listing[jax.random.permutation(jax.random.fold_in(own, 1), rows)]
    turn = jax.random.randint(jax.random.fold_in(own, 2), (rows, 1), 0, top)
    return jnp.take_along_axis(listing, (jnp.arange(top)[None, :] + turn) % top, axis=1)


def shares(amount, total, limit, skew, full):
    portions = [(1 << 20) // math.isqrt(standing ** skew) + 1 for standing in range(1, amount + 1)]
    largest = limit if full else min(limit, max(-(-total // amount), total * portions[0] // sum(portions)))
    least = 1 if total - largest >= amount - 1 else 0
    holding, surplus = [largest] + [least] * (amount - 1), total - largest - least * (amount - 1)
    while surplus > 0:
        movable = [i for i in range(1, amount) if holding[i] < largest] or [i for i in range(1, amount) if holding[i] < limit]
        whole, remaining = sum([portions[i] for i in movable]), surplus
        for i in movable:
            extra = min(limit - holding[i], max(1, remaining * portions[i] // whole), surplus)
            holding[i] = holding[i] + extra
            surplus = surplus - extra
    return np.array(holding)


def bell_draw(rng, dims, spread, bound, shards=(), held_as=jnp.bfloat16):
    drawn = spread * jax.random.normal(rng, dims, jnp.float32)
    if shards:
        drawn = drawn * shard_levels(rng, dims, shards, -0.22, 0.18)
    return jnp.clip(drawn, -bound, bound).astype(held_as)


def setup_inputs(seed: int = 0) -> dict:
    key_of = jax.random.split(jax.random.key(seed), 9)
    tokens = bell_draw(key_of[0], (TOKENS, MODEL_DIM), 1.0, 6.0, ((0, 8),))
    norm_gain = jnp.clip(1.0 + 0.18 * jax.random.normal(key_of[1], (MODEL_DIM,), jnp.float32), 0.1, 1.9)
    routes_keys = jax.random.split(jax.random.fold_in(key_of[2], 1), TOKENS // TOK_DEV)
    routes_turns = jax.random.permutation(jax.random.fold_in(key_of[2], 3), TOKENS // TOK_DEV)
    routes = jax.vmap(lambda own, number: assign_block(jax.random.fold_in(key_of[2], 2), own, number, TOK_DEV, EXPERTS, TOPK, CAP, 2))(routes_keys, routes_turns).reshape((TOKENS, TOPK))
    group_prob = jnp.clip(0.2 + 0.8 * jax.random.uniform(key_of[3], (TOKENS,), jnp.float32) ** shard_levels(key_of[3], (TOKENS,), ((0, 8),), -0.2, 0.2), 0.2, 1.0)
    expert_logits = bell_draw(key_of[4], (TOKENS, TOPK), 1.5, 6.0, ((0, 8),), jnp.float32)
    gate_weight = bell_draw(key_of[5], (EXPERTS, MODEL_DIM, FF), MODEL_DIM ** -0.5, 0.125, ((0, 8), (2, 4)))
    up_weight = bell_draw(key_of[6], (EXPERTS, MODEL_DIM, FF), MODEL_DIM ** -0.5, 0.125, ((0, 8), (2, 4)))
    down_matrix = bell_draw(key_of[7], (EXPERTS, FF, MODEL_DIM), FF ** -0.5, 0.3125, ((0, 8), (1, 4)))
    return {"tokens": tokens, "norm_gain": norm_gain, "routes": routes, "group_prob": group_prob, "expert_logits": expert_logits, "gate_weight": gate_weight, "up_weight": up_weight, "down_matrix": down_matrix}


def reference(tokens, norm_gain, routes, group_prob, expert_logits, gate_weight, up_weight, down_matrix):
    values = tokens.astype(jnp.float32)
    normed = (values * lax.rsqrt(lax.optimization_barrier(jnp.mean(values * values, -1, keepdims=True)) + 1e-06) * norm_gain).astype(jnp.bfloat16)
    weights = group_prob[:, None] * jax.nn.softmax(expert_logits.astype(jnp.float32), axis=-1)
    flat_ids = routes.reshape(-1)
    flat_weights = weights.reshape(-1)
    upper_limit = N_EP * CAP
    slice_width = FF // N_TP

    def visit(total, expert_index):
        hits = flat_ids == expert_index
        found = jnp.nonzero(hits, size=upper_limit, fill_value=0)[0].astype(jnp.int32)
        usable = jnp.arange(upper_limit, dtype=jnp.int32) < jnp.sum(hits.astype(jnp.int32))
        owners = (found // TOPK).astype(jnp.int32)
        inputs = normed[owners]
        gate_proj = jnp.dot(inputs, gate_weight[expert_index], preferred_element_type=jnp.float32)
        up_proj = jnp.dot(inputs, up_weight[expert_index], preferred_element_type=jnp.float32)
        hidden_state = (jax.nn.silu(gate_proj) * up_proj).astype(jnp.bfloat16)
        block_list = jnp.einsum('lzn,znx->zlx', hidden_state.reshape(upper_limit, N_TP, slice_width).astype(jnp.float32), down_matrix[expert_index].reshape(N_TP, slice_width, MODEL_DIM).astype(jnp.float32)).astype(jnp.bfloat16)
        expert_out = lax.optimization_barrier(jnp.sum(block_list.astype(jnp.float32), 0)).astype(jnp.bfloat16)
        scale = jnp.where(usable, flat_weights[found], jnp.zeros((), jnp.float32))
        total = total.at[owners].add(expert_out.astype(jnp.float32) * scale[:, None])
        return (total, None)
    total, _ = lax.scan(visit, jnp.zeros((TOKENS, MODEL_DIM), jnp.float32), jnp.arange(EXPERTS, dtype=jnp.int32))
    return total.astype(jnp.bfloat16)
```

```python
import functools

import jax
import jax.numpy as jnp
from jax import lax
from jax.experimental import pallas as pl
from jax.experimental.pallas import tpu as pltpu
from jax.sharding import PartitionSpec as P


def hidden_part(buffer, gate_weight, up_weight):
    local_count = gate_weight.shape[0]
    grouped = buffer.reshape(
        buffer.shape[0] // local_count, local_count, buffer.shape[1], buffer.shape[2]
    )
    gate_proj = jnp.einsum(
        "sknd,kdf->sknf", grouped, gate_weight, preferred_element_type=jnp.float32
    )
    up_proj = jnp.einsum("sknd,kdf->sknf", grouped, up_weight, preferred_element_type=jnp.float32)
    hidden_state = (jax.nn.silu(gate_proj) * up_proj).astype(jnp.bfloat16)
    return hidden_state.reshape(buffer.shape[0], buffer.shape[1], hidden_state.shape[3])


def down_blocks(hidden_full, down_cols, block_count):
    local_count = down_cols.shape[0]
    width = hidden_full.shape[2] // block_count
    grouped = hidden_full.reshape(
        hidden_full.shape[0] // local_count, local_count, hidden_full.shape[1], block_count, width
    )
    columns = down_cols.reshape(local_count, block_count, width, down_cols.shape[2])
    block_list = jnp.einsum(
        "sknrf,krfd->sknrd", grouped, columns, preferred_element_type=jnp.float32
    ).astype(jnp.bfloat16)
    summed = jnp.sum(block_list.astype(jnp.float32), 3).astype(jnp.bfloat16)
    return summed.reshape(hidden_full.shape[0], hidden_full.shape[1], down_cols.shape[2])


def body(tokens, norm_gain, routes, group_prob, expert_logits, gate_weight, up_weight, down_matrix):
    tok_rows, model_width = tokens.shape
    top_count = routes.shape[1]
    experts = gate_weight.shape[0] * lax.axis_size("ep")
    capacity = 3 * top_count * tok_rows // (2 * experts)
    block_count = lax.axis_size("tp")
    down_cols = lax.all_to_all(down_matrix, "tp", split_axis=2, concat_axis=1, tiled=True)
    values = tokens.astype(jnp.float32)
    normed = (
        values * lax.rsqrt(jnp.mean(values * values, -1, keepdims=True) + 1e-06) * norm_gain
    ).astype(jnp.bfloat16)
    flat_ids = routes.reshape(-1)
    onehot = (flat_ids[:, None] == jnp.arange(experts, dtype=jnp.int32)[None, :]).astype(jnp.int32)
    earlier = jnp.cumsum(onehot, 0) - onehot
    slot_index = jnp.sum(earlier * onehot, 1)
    target = flat_ids * capacity + slot_index
    owners = jnp.arange(tok_rows * top_count, dtype=jnp.int32) // top_count
    outgoing = (
        jnp.zeros((experts * capacity, model_width), jnp.bfloat16).at[target].set(normed[owners])
    )
    outgoing = outgoing.reshape(experts, capacity, model_width)
    hidden_state = hidden_part(
        lax.all_to_all(outgoing, "ep", split_axis=0, concat_axis=0, tiled=True),
        gate_weight,
        up_weight,
    )
    hidden_full = lax.all_gather(hidden_state, "tp", axis=2, tiled=True)
    summed = down_blocks(hidden_full, down_cols, block_count)
    returned = lax.all_to_all(summed, "ep", split_axis=0, concat_axis=0, tiled=True)
    flat_back = returned.reshape(experts * capacity, returned.shape[2])
    weights = group_prob[:, None] * jax.nn.softmax(expert_logits, axis=-1)
    picked = flat_back[target].reshape(tok_rows, top_count, flat_back.shape[1]).astype(jnp.float32)
    combined = jnp.sum(picked * weights[:, :, None], 1).astype(jnp.bfloat16)
    return combined


MESH = pl.DeviceIdType.MESH
F32, BF16 = jnp.float32, jnp.bfloat16


def round_up(value, step):
    return -(-value // step) * step


def toggled(index, mask):
    bit = 1
    result = index
    while bit <= mask:
        if mask & bit:
            result = result + bit * (1 - 2 * ((index // bit) % 2))
        bit *= 2
    return result


def expert_kernel(
    n_ep, n_tp, capacity, width,
    tokens_hbm, gain_hbm, routes_hbm, prob_hbm, logits_hbm, gate_ref, up_ref, down_ref,
    out_ref,
    tokens_ref, gain_ref, routes_ref, prob_ref, logits_ref, load_sem, normed, select, weigh, outgoing, arrived, gate_up, down_cols, hidden, result, returned,
    send_disp, recv_disp, send_core, recv_core, send_side, recv_side, send_relay, recv_relay,
    send_down, recv_down, send_hid, recv_hid, send_back, recv_back,
):
    loads = [
        pltpu.make_async_copy(source, target, load_sem.at[i])
        for i, (source, target) in enumerate((
            (routes_hbm, routes_ref), (tokens_hbm, tokens_ref), (gain_hbm, gain_ref),
            (prob_hbm, prob_ref), (logits_hbm, logits_ref),
        ))
    ]
    for load in loads:
        load.start()
    rows, model = tokens_ref.shape
    quarter = model // n_tp
    fpad = gate_up.shape[0] // 2
    n_hi = n_tp // 2
    slots = n_ep * capacity
    e = lax.axis_index("ep")
    t = lax.axis_index("tp")
    partner = t + 1 - 2 * (t % 2)

    def over(index, h):
        return (index + 2 * h) % n_tp

    def back(index, h):
        return (index + n_tp - 2 * h) % n_tp

    barrier = pltpu.get_barrier_semaphore()
    for r in range(1, n_ep):
        pl.semaphore_signal(barrier, inc=1, device_id={"ep": toggled(e, r), "tp": t}, device_id_type=MESH)
    for j in range(1, n_tp):
        pl.semaphore_signal(barrier, inc=1, device_id={"ep": e, "tp": (t + j) % n_tp}, device_id_type=MESH)

    fetch_gate = pltpu.make_async_copy(gate_ref, gate_up.at[pl.ds(0, width)], load_sem.at[5])
    fetch_up = pltpu.make_async_copy(up_ref, gate_up.at[pl.ds(fpad, width)], load_sem.at[6])
    fetch_down = pltpu.make_async_copy(
        down_ref.at[:, pl.ds(pl.multiple_of(t * quarter, quarter), quarter)],
        down_cols.at[t, pl.ds(0, width)], load_sem.at[7])
    fetches = [fetch_gate, fetch_up, fetch_down]
    for fetch in fetches:
        fetch.start()
    for load in loads:
        load.wait()

    first, second = routes_ref[0:1, :], routes_ref[1:2, :]
    lanes = round_up(n_ep, 16)
    expert_row = lax.broadcasted_iota(jnp.int32, (lanes, rows), 0)
    hit0 = (expert_row == first).astype(F32)
    hit1 = (expert_row == second).astype(F32)
    before = (
        lax.broadcasted_iota(jnp.int32, (rows, rows), 0) < lax.broadcasted_iota(jnp.int32, (rows, rows), 1)
    ).astype(F32).astype(BF16)
    earlier = jnp.dot((hit0 + hit1).astype(BF16), before, preferred_element_type=F32)
    slot0 = jnp.sum(earlier * hit0, 0, keepdims=True)
    slot1 = jnp.sum(earlier * hit1, 0, keepdims=True)
    place0 = first * capacity + slot0.astype(jnp.int32)
    place1 = second * capacity + slot1.astype(jnp.int32)
    slot_row = lax.broadcasted_iota(jnp.int32, (slots, rows), 0)
    at0, at1 = slot_row == place0, slot_row == place1
    select[...] = (at0.astype(F32) + at1.astype(F32)).astype(BF16)

    values = tokens_ref[...].astype(F32)
    scale = lax.rsqrt(jnp.mean(values * values, -1, keepdims=True) + 1e-06)
    normed[...] = (values * scale * gain_ref[...]).astype(BF16)

    for h in range(n_hi):
        part = normed[:, pl.ds(pl.multiple_of(back(t, h) * quarter, quarter), quarter)]
        packed = jnp.dot(select[...], part, preferred_element_type=F32).astype(BF16)
        outgoing[h] = packed.reshape(n_ep, capacity, quarter)

    pl.semaphore_wait(barrier, n_ep - 1 + n_tp - 1)

    def disp(r, h=0):
        peer = toggled(e, r)
        origin = back(t, h)
        return pltpu.make_async_remote_copy(
            src_ref=outgoing.at[h, peer], dst_ref=arrived.at[r, origin],
            send_sem=send_disp.at[r, h], recv_sem=recv_disp.at[r, h],
            device_id={"ep": peer, "tp": t}, device_id_type=MESH)

    def core(r):
        return pltpu.make_async_remote_copy(
            src_ref=arrived.at[r, t], dst_ref=arrived.at[r, t], send_sem=send_core.at[r], recv_sem=recv_core.at[r],
            device_id={"ep": e, "tp": partner}, device_id_type=MESH)

    def side(r, h):
        return pltpu.make_async_remote_copy(
            src_ref=arrived.at[r, t], dst_ref=arrived.at[r, t], send_sem=send_side.at[r, h], recv_sem=recv_side.at[r, h],
            device_id={"ep": e, "tp": over(t, h)}, device_id_type=MESH)

    def relay(r, h):
        origin = back(t, h)
        return pltpu.make_async_remote_copy(
            src_ref=arrived.at[r, origin], dst_ref=arrived.at[r, origin],
            send_sem=send_relay.at[r, h], recv_sem=recv_relay.at[r, h],
            device_id={"ep": e, "tp": partner}, device_id_type=MESH)

    def down(j):
        peer = (t + j) % n_tp
        return pltpu.make_async_remote_copy(
            src_ref=down_ref.at[:, pl.ds(pl.multiple_of(peer * quarter, quarter), quarter)],
            dst_ref=down_cols.at[t, pl.ds(0, width)], send_sem=send_down.at[j], recv_sem=recv_down.at[j],
            device_id={"ep": e, "tp": peer}, device_id_type=MESH)

    def hid(p, j):
        return pltpu.make_async_remote_copy(
            src_ref=hidden.at[p, t], dst_ref=hidden.at[p, t], send_sem=send_hid.at[p, j], recv_sem=recv_hid.at[p, j],
            device_id={"ep": e, "tp": (t + j) % n_tp}, device_id_type=MESH)

    def home(r):
        return pltpu.make_async_remote_copy(
            src_ref=result.at[r], dst_ref=returned.at[e], send_sem=send_back.at[r], recv_sem=recv_back.at[r],
            device_id={"ep": toggled(e, r), "tp": t}, device_id_type=MESH)

    def landed(ref, sem):
        pltpu.make_async_copy(ref, ref, sem).wait()

    near = range(1, n_ep // 2)
    far = range(max(1, n_ep // 2), n_ep)
    for r in near:
        for h in range(n_hi):
            disp(r, h).start()
    for r in far:
        disp(r).start()
    for j in range(1, n_tp):
        down(j).start()

    if fpad > width:
        gate_up[width:fpad] = jnp.zeros((fpad - width, model), BF16)
        gate_up[fpad + width:] = jnp.zeros((fpad - width, model), BF16)
        down_cols[:, width:fpad] = jnp.zeros((n_tp, fpad - width, quarter), BF16)

    logit0, logit1 = logits_ref[0:1, :], logits_ref[1:2, :]
    top = jnp.maximum(logit0, logit1)
    exp0, exp1 = jnp.exp(logit0 - top), jnp.exp(logit1 - top)
    share = prob_ref[...] / (exp0 + exp1)
    weight = (jnp.where(at0, share * exp0, 0.0) + jnp.where(at1, share * exp1, 0.0)).T
    high = weight.astype(BF16)
    weigh[0] = high
    weigh[1] = (weight - high.astype(F32)).astype(BF16)

    def product(left, right):
        return lax.dot_general(left, right, (((1,), (1,)), ((), ())), preferred_element_type=F32)

    def take(r):
        landed(arrived.at[r, t], recv_disp.at[r, 0])
        if r in far:
            for h in range(1, n_hi):
                side(r, h).start()
        core(r).start()
        if r in near:
            for h in range(1, n_hi):
                landed(arrived.at[r, back(t, h)], recv_disp.at[r, h])
                relay(r, h).start()

    def pass_on(r):
        for h in range(1, n_hi):
            landed(arrived.at[r, back(t, h)], recv_side.at[r, h])
            relay(r, h).start()

    def expand(p):
        for r in (2 * p, 2 * p + 1):
            if r:
                landed(arrived.at[r, partner], recv_core.at[r])
                for h in range(1, n_hi):
                    landed(arrived.at[r, back(partner, h)], recv_relay.at[r, h])
            else:
                own = select[pl.ds(pl.multiple_of(e * capacity, capacity), capacity)]
                for q in range(n_tp):
                    block = jnp.dot(own, normed[:, q * quarter:(q + 1) * quarter], preferred_element_type=F32)
                    arrived[0, q] = block.astype(BF16)
        acc = jnp.zeros((2 * capacity, 2 * fpad), F32)
        for q in range(n_tp):
            block = arrived[2 * p:2 * p + 2, q].reshape(2 * capacity, quarter)
            acc = acc + product(block, gate_up[:, q * quarter:(q + 1) * quarter])
        gate, up = acc[:, :fpad], acc[:, fpad:]
        hidden[p, t] = (gate / (1.0 + jnp.exp(-gate)) * up).astype(BF16)
        for j in range(1, n_tp):
            hid(p, j).start()

    def contract(p):
        for j in range(1, n_tp):
            landed(hidden.at[p, (t + n_tp - j) % n_tp], recv_hid.at[p, j])
        acc = jnp.zeros((2 * capacity, quarter), F32)
        for q in range(n_tp):
            acc = acc + jnp.dot(hidden[p, q], down_cols[q], preferred_element_type=F32)
        for i in range(2):
            r = 2 * p + i
            block = acc[i * capacity:(i + 1) * capacity].astype(BF16)
            if r:
                result[r] = block
                home(r).start()
            else:
                returned[e] = block

    for fetch in fetches:
        fetch.wait()
    pairs = n_ep // 2
    todo = []
    for p in range(pairs):
        rounds = [r for r in (2 * p, 2 * p + 1) if r]
        todo.append((3 * p, take, rounds))
        todo.append((3 * p + 3, pass_on, [r for r in rounds if r in far]))
        todo.append((3 * p + 4 if rounds[0] in far else 3 * p + 2, expand, [p]))
        todo.append((3 * p + 8 if rounds[0] in far else 3 * p + 6, contract, [p]))
    todo.sort(key=lambda entry: entry[0])
    waited = False
    for _, stage, items in todo:
        if stage is contract and not waited:
            waited = True
            for j in range(1, n_tp):
                landed(down_cols.at[(t + n_tp - j) % n_tp, pl.ds(0, width)], recv_down.at[j])
        for item in items:
            stage(item)

    for r in range(1, n_ep):
        landed(returned.at[toggled(e, r)], recv_back.at[r])
    back_rows = returned[...].reshape(slots, quarter)
    total = jnp.dot(weigh[0], back_rows, preferred_element_type=F32)
    total = total + jnp.dot(weigh[1], back_rows, preferred_element_type=F32)
    out_ref[...] = total.astype(BF16)

    for r in range(1, n_ep):
        disp(r).wait_send()
        core(r).wait_send()
        home(r).wait_send()
        for h in range(1, n_hi):
            if r in near:
                disp(r, h).wait_send()
            else:
                side(r, h).wait_send()
            relay(r, h).wait_send()
    for j in range(1, n_tp):
        down(j).wait_send()
        for p in range(pairs):
            hid(p, j).wait_send()


def fused_body(tokens, norm_gain, routes, group_prob, expert_logits, gate_weight, up_weight, down_matrix):
    n_ep, n_tp = lax.axis_size("ep"), lax.axis_size("tp")
    rows, model = tokens.shape
    capacity = 3 * routes.shape[1] * rows // (2 * n_ep)
    width = gate_weight.shape[2]
    fpad = round_up(width, 128)
    quarter = model // n_tp
    n_hi = n_tp // 2
    sem = pltpu.SemaphoreType.DMA
    vmem = pl.BlockSpec(memory_space=pltpu.VMEM)
    return pl.pallas_call(
        functools.partial(expert_kernel, n_ep, n_tp, capacity, width),
        out_shape=jax.ShapeDtypeStruct((rows, quarter), BF16),
        in_specs=[pl.BlockSpec(memory_space=pl.ANY)] * 8,
        out_specs=vmem,
        scratch_shapes=[
            pltpu.VMEM((rows, model), BF16),
            pltpu.VMEM((1, model), F32),
            pltpu.VMEM((2, rows), jnp.int32),
            pltpu.VMEM((1, rows), F32),
            pltpu.VMEM((2, rows), F32),
            sem((8,)),
            pltpu.VMEM((rows, model), BF16),
            pltpu.VMEM((n_ep * capacity, rows), BF16),
            pltpu.VMEM((2, rows, n_ep * capacity), BF16),
            pltpu.VMEM((n_hi, n_ep, capacity, quarter), BF16),
            pltpu.VMEM((n_ep, n_tp, capacity, quarter), BF16),
            pltpu.VMEM((2 * fpad, model), BF16),
            pltpu.VMEM((n_tp, fpad, quarter), BF16),
            pltpu.VMEM((n_ep // 2, n_tp, 2 * capacity, fpad), BF16),
            pltpu.VMEM((n_ep, capacity, quarter), BF16),
            pltpu.VMEM((n_ep, capacity, quarter), BF16),
            sem((n_ep, n_hi)), sem((n_ep, n_hi)),
            sem((n_ep,)), sem((n_ep,)),
            sem((n_ep, n_hi)), sem((n_ep, n_hi)),
            sem((n_ep, n_hi)), sem((n_ep, n_hi)),
            sem((n_tp,)), sem((n_tp,)),
            sem((n_ep, n_tp)), sem((n_ep, n_tp)),
            sem((n_ep,)), sem((n_ep,)),
        ],
        compiler_params=pltpu.CompilerParams(collective_id=0, has_side_effects=True, vmem_limit_bytes=32 * 1024 * 1024),
    )(*[pltpu.with_memory_space_constraint(array, pltpu.HBM) for array in (
        tokens, norm_gain.reshape(1, model), routes.T, group_prob.reshape(1, rows), expert_logits.T,
        gate_weight.reshape(model, width).T, up_weight.reshape(model, width).T, down_matrix.reshape(width, model),
    )])


def fits_kernel(n_ep, n_tp, rows, experts, top, model):
    capacity = 3 * top * rows // (2 * experts)
    return (
        experts == n_ep and top == 2 and n_ep & (n_ep - 1) == 0 and n_ep <= 16 and n_tp % 2 == 0
        and capacity % 16 == 0 and rows % 128 == 0 and model % (128 * n_tp) == 0
    )


def solution(mesh):
    n_ep, n_tp = mesh.shape["ep"], mesh.shape["tp"]

    def chosen(*arrays):
        rows, model = arrays[0].shape
        fits = fits_kernel(n_ep, n_tp, rows, arrays[5].shape[0] * n_ep, arrays[2].shape[1], model)
        return (fused_body if fits else body)(*arrays)

    return jax.shard_map(
        chosen,
        mesh=mesh,
        in_specs=(
            P("ep", None),
            P(),
            P("ep", None),
            P("ep"),
            P("ep", None),
            P("ep", None, "tp"),
            P("ep", None, "tp"),
            P("ep", "tp", None),
        ),
        out_specs=P("ep", "tp"),
        check_vma=False,
    )
```

```python
import functools

import jax
import jax.numpy as jnp
from jax import lax
from jax.experimental import pallas as pl
from jax.experimental.pallas import tpu as pltpu
from jax.sharding import PartitionSpec as P


def hidden_part(buffer, gate_weight, up_weight):
    local_count = gate_weight.shape[0]
    grouped = buffer.reshape(
        buffer.shape[0] // local_count, local_count, buffer.shape[1], buffer.shape[2]
    )
    gate_proj = jnp.einsum(
        "sknd,kdf->sknf", grouped, gate_weight, preferred_element_type=jnp.float32
    )
    up_proj = jnp.einsum("sknd,kdf->sknf", grouped, up_weight, preferred_element_type=jnp.float32)
    hidden_state = (jax.nn.silu(gate_proj) * up_proj).astype(jnp.bfloat16)
    return hidden_state.reshape(buffer.shape[0], buffer.shape[1], hidden_state.shape[3])


def down_blocks(hidden_full, down_cols, block_count):
    local_count = down_cols.shape[0]
    width = hidden_full.shape[2] // block_count
    grouped = hidden_full.reshape(
        hidden_full.shape[0] // local_count, local_count, hidden_full.shape[1], block_count, width
    )
    columns = down_cols.reshape(local_count, block_count, width, down_cols.shape[2])
    block_list = jnp.einsum(
        "sknrf,krfd->sknrd", grouped, columns, preferred_element_type=jnp.float32
    ).astype(jnp.bfloat16)
    summed = jnp.sum(block_list.astype(jnp.float32), 3).astype(jnp.bfloat16)
    return summed.reshape(hidden_full.shape[0], hidden_full.shape[1], down_cols.shape[2])


def body(tokens, norm_gain, routes, group_prob, expert_logits, gate_weight, up_weight, down_matrix):
    tok_rows, model_width = tokens.shape
    top_count = routes.shape[1]
    experts = gate_weight.shape[0] * lax.axis_size("ep")
    capacity = 3 * top_count * tok_rows // (2 * experts)
    block_count = lax.axis_size("tp")
    down_cols = lax.all_to_all(down_matrix, "tp", split_axis=2, concat_axis=1, tiled=True)
    values = tokens.astype(jnp.float32)
    normed = (
        values * lax.rsqrt(jnp.mean(values * values, -1, keepdims=True) + 1e-06) * norm_gain
    ).astype(jnp.bfloat16)
    flat_ids = routes.reshape(-1)
    onehot = (flat_ids[:, None] == jnp.arange(experts, dtype=jnp.int32)[None, :]).astype(jnp.int32)
    earlier = jnp.cumsum(onehot, 0) - onehot
    slot_index = jnp.sum(earlier * onehot, 1)
    target = flat_ids * capacity + slot_index
    owners = jnp.arange(tok_rows * top_count, dtype=jnp.int32) // top_count
    outgoing = (
        jnp.zeros((experts * capacity, model_width), jnp.bfloat16).at[target].set(normed[owners])
    )
    outgoing = outgoing.reshape(experts, capacity, model_width)
    hidden_state = hidden_part(
        lax.all_to_all(outgoing, "ep", split_axis=0, concat_axis=0, tiled=True),
        gate_weight,
        up_weight,
    )
    hidden_full = lax.all_gather(hidden_state, "tp", axis=2, tiled=True)
    summed = down_blocks(hidden_full, down_cols, block_count)
    returned = lax.all_to_all(summed, "ep", split_axis=0, concat_axis=0, tiled=True)
    flat_back = returned.reshape(experts * capacity, returned.shape[2])
    weights = group_prob[:, None] * jax.nn.softmax(expert_logits, axis=-1)
    picked = flat_back[target].reshape(tok_rows, top_count, flat_back.shape[1]).astype(jnp.float32)
    combined = jnp.sum(picked * weights[:, :, None], 1).astype(jnp.bfloat16)
    return combined


MESH = pl.DeviceIdType.MESH
F32, BF16 = jnp.float32, jnp.bfloat16


def round_up(value, step):
    return -(-value // step) * step


def SCOPE(name, run):
    run()


def flipped(index, bit):
    return bit * (1 - 2 * ((index // bit) % 2))


def toggled(index, mask):
    result, bit = index, 1
    while bit <= mask:
        if mask & bit:
            result = result + flipped(index, bit)
        bit *= 2
    return result


def expert_kernel(
    n_ep, capacity, width,
    tokens_hbm, gain_hbm, routes_hbm, prob_hbm, logits_hbm, gate_ref, up_ref, down_ref,
    out_ref,
    tokens_ref, gain_ref, routes_ref, prob_ref, logits_ref, normed, select, weigh, outgoing, arrived, gate_up, down_rows,
    hidden, result, returned,
    load_sem, send_disp, recv_disp, send_side, recv_side, send_hid, recv_hid, send_home, recv_home, send_weight, recv_weight,
):
    loads = [
        pltpu.make_async_copy(source, target, load_sem.at[i])
        for i, (source, target) in enumerate((
            (routes_hbm, routes_ref), (tokens_hbm, tokens_ref), (gain_hbm, gain_ref),
            (prob_hbm, prob_ref), (logits_hbm, logits_ref),
        ))
    ]
    for load in loads:
        load.start()
    rows, model = tokens_ref.shape
    half, quarter = model // 2, model // 4
    fpad = gate_up.shape[2]
    slots = n_ep * capacity
    e = lax.axis_index("ep")
    t = lax.axis_index("tp")
    x, c = t // 2, t % 2
    partner, across = t + 1 - 2 * c, (t + 2) % 4
    outer = 1 - ((e // 2) % 2 + (e // 4) % 2) % 2

    barrier = pltpu.get_barrier_semaphore()
    for r in range(n_ep):
        for mate in (t, partner):
            if r or mate is partner:
                pl.semaphore_signal(
                    barrier, inc=1, device_id={"ep": toggled(e, r), "tp": mate}, device_id_type=MESH)
    pl.semaphore_signal(barrier, inc=1, device_id={"ep": e, "tp": across}, device_id_type=MESH)

    columns = pl.ds(pl.multiple_of(x * half, half), half)
    fetches = [
        pltpu.make_async_copy(gate_ref, gate_up.at[0, c, pl.ds(0, width)], load_sem.at[5]),
        pltpu.make_async_copy(up_ref, gate_up.at[1, c, pl.ds(0, width)], load_sem.at[6]),
        pltpu.make_async_copy(down_ref.at[:, columns], down_rows.at[x, c, pl.ds(0, width)], load_sem.at[7]),
    ]
    for fetch in fetches:
        fetch.start()
    SCOPE("w_loads", lambda: [load.wait() for load in loads])

    first, second = routes_ref[0:1, :], routes_ref[1:2, :]
    lanes = round_up(n_ep, 16)
    expert_row = lax.broadcasted_iota(jnp.int32, (lanes, rows), 0)
    hit0 = (expert_row == first).astype(F32)
    hit1 = (expert_row == second).astype(F32)
    before = (
        lax.broadcasted_iota(jnp.int32, (rows, rows), 0) < lax.broadcasted_iota(jnp.int32, (rows, rows), 1)
    ).astype(F32).astype(BF16)
    earlier = jnp.dot((hit0 + hit1).astype(BF16), before, preferred_element_type=F32)
    slot0 = jnp.sum(earlier * hit0, 0, keepdims=True)
    slot1 = jnp.sum(earlier * hit1, 0, keepdims=True)
    place0 = (first ^ e) * capacity + slot0.astype(jnp.int32)
    place1 = (second ^ e) * capacity + slot1.astype(jnp.int32)
    slot_row = lax.broadcasted_iota(jnp.int32, (slots, rows), 0)
    at0, at1 = slot_row == place0, slot_row == place1
    select[...] = (at0.astype(F32) + at1.astype(F32)).astype(BF16)

    values = tokens_ref[...].astype(F32)
    scale = lax.rsqrt(jnp.mean(values * values, -1, keepdims=True) + 1e-06)
    normed[...] = (values * scale * gain_ref[...]).astype(BF16)

    for h in range(2):
        part = normed[:, pl.ds(pl.multiple_of(((t + 2 * h) % 4) * quarter, quarter), quarter)]
        packed = jnp.dot(select[...], part, preferred_element_type=F32).astype(BF16)
        outgoing[h] = packed.reshape(n_ep, capacity, quarter)

    SCOPE("w_barrier", lambda: pl.semaphore_wait(barrier, 2 * n_ep))

    def remote(source, target, send, recv, ep, tp):
        return pltpu.make_async_remote_copy(
            src_ref=source, dst_ref=target, send_sem=send, recv_sem=recv,
            device_id={"ep": ep, "tp": tp}, device_id_type=MESH)

    def landed(ref, sem):
        pltpu.make_async_copy(ref, ref, sem).wait()

    own_half = pl.ds(2 * x, 2)
    for r in range(1, n_ep // 2):
        for h in range(2):
            remote(
                outgoing.at[h, r], arrived.at[r // 2, (t + 2 * h) % 4], send_disp.at[0], recv_disp.at[r // 2],
                toggled(e, r), 2 * x + r % 2).start()
    for far in (outer, 1 - outer):
        for odd in range(2):
            peer = e + flipped(e, 4) + far * flipped(e, 2) + odd * flipped(e, 1)
            remote(
                outgoing.at[0, 4 + 2 * far + odd], arrived.at[2 + far, t], send_disp.at[0], recv_disp.at[2 + far],
                peer, 2 * x + odd).start()
    other = pl.ds(pl.multiple_of((1 - x) * half, half), half)
    shares = [
        remote(down_ref.at[:, other], down_rows.at[x, c, pl.ds(0, width)], send_weight.at[0], recv_weight.at[0], e, across),
        remote(gate_ref, gate_up.at[0, c, pl.ds(0, width)], send_weight.at[1], recv_weight.at[1], e, partner),
        remote(up_ref, gate_up.at[1, c, pl.ds(0, width)], send_weight.at[2], recv_weight.at[2], e, partner),
        remote(down_ref.at[:, columns], down_rows.at[x, c, pl.ds(0, width)], send_weight.at[3], recv_weight.at[3], e, partner),
    ]
    for share in shares:
        share.start()
    far_rows = down_rows.at[1 - x, c, pl.ds(0, width)]
    relay = remote(far_rows, far_rows, send_weight.at[4], recv_weight.at[4], e, partner)

    if fpad > width:
        gate_up[:, :, width:fpad] = jnp.zeros((2, 2, fpad - width, model), BF16)
        down_rows[:, :, width:fpad] = jnp.zeros((2, 2, fpad - width, half), BF16)

    logit0, logit1 = logits_ref[0:1, :], logits_ref[1:2, :]
    top = jnp.maximum(logit0, logit1)
    exp0, exp1 = jnp.exp(logit0 - top), jnp.exp(logit1 - top)
    share = prob_ref[...] / (exp0 + exp1)
    weight = jnp.where(at0, share * exp0, 0.0) + jnp.where(at1, share * exp1, 0.0)
    for part in range(2):
        turned = weight[part * (slots // 2):(part + 1) * (slots // 2)].T
        high = turned.astype(BF16)
        weigh[part, 0] = high
        weigh[part, 1] = (turned - high.astype(F32)).astype(BF16)

    def product(left, right):
        return lax.dot_general(left, right, (((1,), (1,)), ((), ())), preferred_element_type=F32)

    def expand(s):
        acc = jnp.zeros((capacity, 4 * fpad), F32)
        for q in range(4):
            columns = gate_up[:, :, :, q * quarter:(q + 1) * quarter].reshape(4 * fpad, quarter)
            acc = acc + product(arrived[s, q], columns)
        gate, up = acc[:, :2 * fpad], acc[:, 2 * fpad:]
        hidden[s, x] = (gate / (1.0 + jnp.exp(-gate)) * up).astype(BF16)
        remote(hidden.at[s, x], hidden.at[s, x], send_hid.at[0], recv_hid.at[s], e, across).start()

    def contract(s):
        SCOPE(f"w_hid{s if isinstance(s, int) else 'f'}", lambda: landed(hidden.at[s, 1 - x], recv_hid.at[s]))
        acc = jnp.zeros((capacity, half), F32)
        for side in range(2):
            acc = acc + jnp.dot(hidden[s, side], down_rows[side].reshape(2 * fpad, half), preferred_element_type=F32)
        for j in range(2):
            result[s, j] = acc[:, j * quarter:(j + 1) * quarter].astype(BF16)

    def take(s):
        mine = arrived.at[s, own_half]
        SCOPE("w_take", lambda: landed(mine, recv_disp.at[s]))
        remote(mine, mine, send_side.at[0], recv_side.at[s - 2], e, across).start()

    def expand_far(s):
        SCOPE("w_side", lambda: landed(arrived.at[s, pl.ds(2 * (1 - x), 2)], recv_side.at[s - 2]))
        expand(s)

    def contract_far(s):
        contract(s)
        odd = c
        peer = e + flipped(e, 4) + (s - 2) * flipped(e, 2) + odd * flipped(e, 1)
        for j in range(2):
            remote(result.at[s, j], returned.at[2 * s + c], send_home.at[1], recv_home.at[2], peer, 2 * x + j).start()

    @pl.when(c == 0)
    def _():
        own = select[0:capacity]
        for q in range(4):
            block = jnp.dot(own, normed[:, q * quarter:(q + 1) * quarter], preferred_element_type=F32)
            arrived[0, q] = block.astype(BF16)

    def weights_ready():
        for fetch in fetches:
            fetch.wait()
        for kind in range(2):
            landed(gate_up.at[kind, 1 - c, pl.ds(0, width)], recv_weight.at[1 + kind])

    SCOPE("w_weights", weights_ready)

    @pl.when(c == 1)
    def _():
        SCOPE("w_near0", lambda: landed(arrived.at[0], recv_disp.at[0]))

    sa, sb = 3 - outer, 2 + outer
    SCOPE("expand0", lambda: expand(0))
    SCOPE("take_a", lambda: take(sa))
    SCOPE("w_near1", lambda: landed(arrived.at[1], recv_disp.at[1]))
    SCOPE("expand1", lambda: expand(1))

    def relay_down():
        landed(far_rows, recv_weight.at[0])
        relay.start()

    SCOPE("relay_down", relay_down)
    SCOPE("expand_a", lambda: expand_far(sa))
    SCOPE("take_b", lambda: take(sb))

    def down_ready():
        landed(down_rows.at[x, 1 - c, pl.ds(0, width)], recv_weight.at[3])
        landed(down_rows.at[1 - x, 1 - c, pl.ds(0, width)], recv_weight.at[4])

    SCOPE("w_down", down_ready)

    def near_home(s):
        contract(s)
        peer = e + (s * flipped(e, 2) if s else 0) + c * flipped(e, 1)
        if s:
            for j in range(2):
                remote(result.at[s, j], returned.at[2 * s + c], send_home.at[0], recv_home.at[1], peer, 2 * x + j).start()
            return

        @pl.when(c == 0)
        def _():
            returned[0] = result[0, 0]
            remote(result.at[0, 1], returned.at[0], send_home.at[2], recv_home.at[0], e, partner).start()

        @pl.when(c == 1)
        def _():
            for j in range(2):
                remote(result.at[0, j], returned.at[1], send_home.at[2], recv_home.at[1], peer, 2 * x + j).start()

    SCOPE("contract0", lambda: near_home(0))
    SCOPE("contract1", lambda: near_home(1))
    SCOPE("contract_a", lambda: contract_far(sa))
    SCOPE("expand_b", lambda: expand_far(sb))
    SCOPE("contract_b", lambda: contract_far(sb))

    def merge(part):
        back = returned[part * (n_ep // 2):(part + 1) * (n_ep // 2)].reshape(slots // 2, quarter)
        return (jnp.dot(weigh[part, 0], back, preferred_element_type=F32)
                + jnp.dot(weigh[part, 1], back, preferred_element_type=F32))

    @pl.when(c == 1)
    def _():
        SCOPE("w_back0", lambda: landed(returned.at[0], recv_home.at[0]))

    SCOPE("w_back1", lambda: landed(returned.at[pl.ds(1, n_ep // 2 - 1)], recv_home.at[1]))
    total = merge(0)
    SCOPE("w_back2", lambda: landed(returned.at[pl.ds(n_ep // 2, n_ep // 2)], recv_home.at[2]))
    out_ref[...] = (total + merge(1)).astype(BF16)

    def finish():
        landed(outgoing.at[:, pl.ds(0, (3 * n_ep // 2 - 2) // 2)], send_disp.at[0])
        landed(arrived.at[pl.ds(0, 2), own_half], send_side.at[0])
        landed(hidden.at[:, x], send_hid.at[0])
        landed(result.at[1], send_home.at[0])
        landed(result.at[pl.ds(2, 2)], send_home.at[1])

        @pl.when(c == 0)
        def _():
            landed(result.at[0, 1], send_home.at[2])

        @pl.when(c == 1)
        def _():
            landed(result.at[0], send_home.at[2])

        for share in shares:
            share.wait_send()
        relay.wait_send()

    SCOPE("w_sends", finish)


def fused_body(tokens, norm_gain, routes, group_prob, expert_logits, gate_weight, up_weight, down_matrix):
    n_ep = lax.axis_size("ep")
    rows, model = tokens.shape
    capacity = 3 * routes.shape[1] * rows // (2 * n_ep)
    width = gate_weight.shape[2]
    fpad = round_up(width, 128)
    half, quarter = model // 2, model // 4
    sem = pltpu.SemaphoreType.DMA
    vmem = pl.BlockSpec(memory_space=pltpu.VMEM)
    operands = (
        tokens, norm_gain.reshape(1, model), routes.T, group_prob.reshape(1, rows), expert_logits.T,
        gate_weight.reshape(model, width).T, up_weight.reshape(model, width).T, down_matrix.reshape(width, model),
    )
    return pl.pallas_call(
        functools.partial(expert_kernel, n_ep, capacity, width),
        out_shape=jax.ShapeDtypeStruct((rows, quarter), BF16),
        in_specs=[pl.BlockSpec(memory_space=pl.ANY)] * 8,
        out_specs=vmem,
        scratch_shapes=[
            pltpu.VMEM((rows, model), BF16),
            pltpu.VMEM((1, model), F32),
            pltpu.VMEM((2, rows), jnp.int32),
            pltpu.VMEM((1, rows), F32),
            pltpu.VMEM((2, rows), F32),
            pltpu.VMEM((rows, model), BF16),
            pltpu.VMEM((n_ep * capacity, rows), BF16),
            pltpu.VMEM((2, 2, rows, n_ep * capacity // 2), BF16),
            pltpu.VMEM((2, n_ep, capacity, quarter), BF16),
            pltpu.VMEM((n_ep // 2, 4, capacity, quarter), BF16),
            pltpu.VMEM((2, 2, fpad, model), BF16),
            pltpu.VMEM((2, 2, fpad, half), BF16),
            pltpu.VMEM((n_ep // 2, 2, capacity, 2 * fpad), BF16),
            pltpu.VMEM((n_ep // 2, 2, capacity, quarter), BF16),
            pltpu.VMEM((n_ep, capacity, quarter), BF16),
            sem((8,)),
            sem((1,)), sem((n_ep // 2,)),
            sem((1,)), sem((2,)),
            sem((1,)), sem((n_ep // 2,)),
            sem((3,)), sem((3,)),
            sem((5,)), sem((5,)),
        ],
        compiler_params=pltpu.CompilerParams(
            collective_id=0, has_side_effects=True, vmem_limit_bytes=32 * 1024 * 1024),
    )(*[pltpu.with_memory_space_constraint(operand, pltpu.HBM) for operand in operands])


def fits_kernel(n_ep, n_tp, rows, experts, top, model):
    capacity = 3 * top * rows // (2 * experts)
    return (
        experts == n_ep and top == 2 and n_ep == 8 and n_tp == 4
        and capacity % 16 == 0 and rows % 128 == 0 and model % 512 == 0
    )


def solution(mesh):
    n_ep, n_tp = mesh.shape["ep"], mesh.shape["tp"]

    def chosen(*arrays):
        rows, model = arrays[0].shape
        fits = fits_kernel(n_ep, n_tp, rows, arrays[5].shape[0] * n_ep, arrays[2].shape[1], model)
        return (fused_body if fits else body)(*arrays)

    return jax.shard_map(
        chosen,
        mesh=mesh,
        in_specs=(
            P("ep", None),
            P(),
            P("ep", None),
            P("ep"),
            P("ep", None),
            P("ep", None, "tp"),
            P("ep", None, "tp"),
            P("ep", "tp", None),
        ),
        out_specs=P("ep", "tp"),
        check_vma=False,
    )
```

```python
import functools

import jax
import jax.numpy as jnp
from jax import lax
from jax.experimental import pallas as pl
from jax.experimental.pallas import tpu as pltpu
from jax.sharding import PartitionSpec as P


def hidden_part(buffer, gate_weight, up_weight):
    local_count = gate_weight.shape[0]
    grouped = buffer.reshape(
        buffer.shape[0] // local_count, local_count, buffer.shape[1], buffer.shape[2]
    )
    gate_proj = jnp.einsum(
        "sknd,kdf->sknf", grouped, gate_weight, preferred_element_type=jnp.float32
    )
    up_proj = jnp.einsum("sknd,kdf->sknf", grouped, up_weight, preferred_element_type=jnp.float32)
    hidden_state = (jax.nn.silu(gate_proj) * up_proj).astype(jnp.bfloat16)
    return hidden_state.reshape(buffer.shape[0], buffer.shape[1], hidden_state.shape[3])


def down_blocks(hidden_full, down_cols, block_count):
    local_count = down_cols.shape[0]
    width = hidden_full.shape[2] // block_count
    grouped = hidden_full.reshape(
        hidden_full.shape[0] // local_count, local_count, hidden_full.shape[1], block_count, width
    )
    columns = down_cols.reshape(local_count, block_count, width, down_cols.shape[2])
    block_list = jnp.einsum(
        "sknrf,krfd->sknrd", grouped, columns, preferred_element_type=jnp.float32
    ).astype(jnp.bfloat16)
    summed = jnp.sum(block_list.astype(jnp.float32), 3).astype(jnp.bfloat16)
    return summed.reshape(hidden_full.shape[0], hidden_full.shape[1], down_cols.shape[2])


def body(tokens, norm_gain, routes, group_prob, expert_logits, gate_weight, up_weight, down_matrix):
    tok_rows, model_width = tokens.shape
    top_count = routes.shape[1]
    experts = gate_weight.shape[0] * lax.axis_size("ep")
    capacity = 3 * top_count * tok_rows // (2 * experts)
    block_count = lax.axis_size("tp")
    down_cols = lax.all_to_all(down_matrix, "tp", split_axis=2, concat_axis=1, tiled=True)
    values = tokens.astype(jnp.float32)
    normed = (
        values * lax.rsqrt(jnp.mean(values * values, -1, keepdims=True) + 1e-06) * norm_gain
    ).astype(jnp.bfloat16)
    flat_ids = routes.reshape(-1)
    onehot = (flat_ids[:, None] == jnp.arange(experts, dtype=jnp.int32)[None, :]).astype(jnp.int32)
    earlier = jnp.cumsum(onehot, 0) - onehot
    slot_index = jnp.sum(earlier * onehot, 1)
    target = flat_ids * capacity + slot_index
    owners = jnp.arange(tok_rows * top_count, dtype=jnp.int32) // top_count
    outgoing = (
        jnp.zeros((experts * capacity, model_width), jnp.bfloat16).at[target].set(normed[owners])
    )
    outgoing = outgoing.reshape(experts, capacity, model_width)
    hidden_state = hidden_part(
        lax.all_to_all(outgoing, "ep", split_axis=0, concat_axis=0, tiled=True),
        gate_weight,
        up_weight,
    )
    hidden_full = lax.all_gather(hidden_state, "tp", axis=2, tiled=True)
    summed = down_blocks(hidden_full, down_cols, block_count)
    returned = lax.all_to_all(summed, "ep", split_axis=0, concat_axis=0, tiled=True)
    flat_back = returned.reshape(experts * capacity, returned.shape[2])
    weights = group_prob[:, None] * jax.nn.softmax(expert_logits, axis=-1)
    picked = flat_back[target].reshape(tok_rows, top_count, flat_back.shape[1]).astype(jnp.float32)
    combined = jnp.sum(picked * weights[:, :, None], 1).astype(jnp.bfloat16)
    return combined


MESH = pl.DeviceIdType.MESH
F32, BF16 = jnp.float32, jnp.bfloat16


def round_up(value, step):
    return -(-value // step) * step


def flipped(index, bit):
    return bit * (1 - 2 * ((index // bit) % 2))


def toggled(index, mask):
    result, bit = index, 1
    while bit <= mask:
        if mask & bit:
            result = result + flipped(index, bit)
        bit *= 2
    return result


def expert_kernel(
    n_ep, capacity, width,
    tokens_hbm, gain_hbm, routes_hbm, prob_hbm, logits_hbm, gate_ref, up_ref, down_ref,
    out_ref,
    tokens_ref, gain_ref, routes_ref, prob_ref, logits_ref, normed, select, weigh, leaving, outgoing, arrived, gate_up,
    down_rows, down_other, hidden, result, returned,
    load_sem, send_disp, recv_disp, send_side, recv_side, send_hid, recv_hid, send_home, recv_home, send_weight, recv_weight,
):
    loads = [
        pltpu.make_async_copy(source, target, load_sem.at[i])
        for i, (source, target) in enumerate((
            (routes_hbm, routes_ref), (tokens_hbm, tokens_ref), (gain_hbm, gain_ref),
            (prob_hbm, prob_ref), (logits_hbm, logits_ref),
        ))
    ]
    for load in loads:
        load.start()
    rows, model = tokens_ref.shape
    half, quarter = model // 2, model // 4
    fpad = gate_up.shape[2]
    near = n_ep // 2
    slots = n_ep * capacity
    e = lax.axis_index("ep")
    t = lax.axis_index("tp")
    x, c = t // 2, t % 2
    partner, across = t + 1 - 2 * c, (t + 2) % 4
    outer = 1 - ((e // 2) % 2 + (e // 4) % 2) % 2

    barrier = pltpu.get_barrier_semaphore()
    for r in reversed(range(n_ep)):
        for mate in (t, partner):
            if r or mate is partner:
                pl.semaphore_signal(
                    barrier, inc=1, device_id={"ep": toggled(e, r), "tp": mate}, device_id_type=MESH)
    pl.semaphore_signal(barrier, inc=1, device_id={"ep": e, "tp": across}, device_id_type=MESH)

    def columns(side):
        return pl.ds(pl.multiple_of(side * half, half), half)

    fetches = [
        pltpu.make_async_copy(down_ref.at[:, columns(1 - x)], down_other, load_sem.at[5]),
        pltpu.make_async_copy(gate_ref, gate_up.at[0, c, pl.ds(0, width)], load_sem.at[6]),
        pltpu.make_async_copy(up_ref, gate_up.at[1, c, pl.ds(0, width)], load_sem.at[7]),
        pltpu.make_async_copy(down_ref.at[:, columns(x)], down_rows.at[x, c, pl.ds(0, width)], load_sem.at[8]),
    ]
    for fetch in fetches:
        fetch.start()
    for load in loads:
        load.wait()

    first, second = routes_ref[0:1, :], routes_ref[1:2, :]
    lanes = round_up(n_ep, 16)
    expert_row = lax.broadcasted_iota(jnp.int32, (lanes, rows), 0)
    hit0 = (expert_row == first).astype(F32)
    hit1 = (expert_row == second).astype(F32)
    before = (
        lax.broadcasted_iota(jnp.int32, (rows, rows), 0) < lax.broadcasted_iota(jnp.int32, (rows, rows), 1)
    ).astype(F32).astype(BF16)
    earlier = jnp.dot((hit0 + hit1).astype(BF16), before, preferred_element_type=F32)
    slot0 = jnp.sum(earlier * hit0, 0, keepdims=True)
    slot1 = jnp.sum(earlier * hit1, 0, keepdims=True)
    place0 = (first ^ e) * capacity + slot0.astype(jnp.int32)
    place1 = (second ^ e) * capacity + slot1.astype(jnp.int32)
    slot_row = lax.broadcasted_iota(jnp.int32, (slots, rows), 0)
    at0, at1 = slot_row == place0, slot_row == place1
    select[...] = (at0.astype(F32) + at1.astype(F32)).astype(BF16)

    values = tokens_ref[...].astype(F32)
    scale = lax.rsqrt(jnp.mean(values * values, -1, keepdims=True) + 1e-06)
    normed[...] = (values * scale * gain_ref[...]).astype(BF16)

    def packed(begin, end, lanes):
        return jnp.dot(
            select[begin * capacity:end * capacity], normed[:, lanes], preferred_element_type=F32
        ).astype(BF16).reshape(end - begin, capacity, half)

    @pl.when(c == 1)
    def _():
        leaving[...] = packed(near, n_ep, columns(x))

    @pl.when(c == 0)
    def _():
        for side in range(2):
            both = packed(0, 2, slice(side * half, (side + 1) * half))
            arrived[0, side] = both[0]
            outgoing[0, side] = both[1]

    pl.semaphore_wait(barrier, 2 * n_ep)

    def remote(source, target, send, recv, ep, tp):
        return pltpu.make_async_remote_copy(
            src_ref=source, dst_ref=target, send_sem=send, recv_sem=recv,
            device_id={"ep": ep, "tp": tp}, device_id_type=MESH)

    def landed(ref, sem):
        pltpu.make_async_copy(ref, ref, sem).wait()

    def far_peer(step, odd):
        return e + flipped(e, 4) + step * flipped(e, 2) + odd * flipped(e, 1)

    @pl.when(c == 1)
    def _():
        for step in (outer, 1 - outer):
            for odd in range(2):
                s = 2 * step + odd
                remote(
                    leaving.at[s], arrived.at[s, x], send_disp.at[0], recv_disp.at[s], far_peer(step, odd), t).start()
        for side in range(2):
            outgoing[0:2, side] = packed(2, 4, slice(side * half, (side + 1) * half))
        for s in (3, 2):
            remote(outgoing.at[s - 2], arrived.at[s], send_disp.at[1], recv_disp.at[s], toggled(e, s), partner).start()

    @pl.when(c == 0)
    def _():
        remote(outgoing.at[0], arrived.at[1], send_disp.at[0], recv_disp.at[1], toggled(e, 1), t).start()

    def owned(ref, side, core):
        return ref.at[side, core, pl.ds(0, width)]

    shares = [
        remote(down_other, owned(down_rows, x, c), send_weight.at[0], recv_weight.at[0], e, across),
        remote(owned(gate_up, 0, c), owned(gate_up, 0, c), send_weight.at[1], recv_weight.at[1], e, partner),
        remote(owned(gate_up, 1, c), owned(gate_up, 1, c), send_weight.at[2], recv_weight.at[2], e, partner),
        remote(owned(down_rows, x, c), owned(down_rows, x, c), send_weight.at[3], recv_weight.at[3], e, partner),
    ]
    for fetch, share in zip(fetches, shares):
        fetch.wait()
        share.start()
    far_rows = owned(down_rows, 1 - x, c)
    relay = remote(far_rows, far_rows, send_weight.at[4], recv_weight.at[4], e, partner)

    if fpad > width:
        gate_up[:, :, width:fpad] = jnp.zeros((2, 2, fpad - width, model), BF16)
        down_rows[:, :, width:fpad] = jnp.zeros((2, 2, fpad - width, half), BF16)

    logit0, logit1 = logits_ref[0:1, :], logits_ref[1:2, :]
    top = jnp.maximum(logit0, logit1)
    exp0, exp1 = jnp.exp(logit0 - top), jnp.exp(logit1 - top)
    share = prob_ref[...] / (exp0 + exp1)
    weight = jnp.where(at0, share * exp0, 0.0) + jnp.where(at1, share * exp1, 0.0)
    for part in range(2):
        turned = weight[part * (slots // 2):(part + 1) * (slots // 2)].T
        high = turned.astype(BF16)
        weigh[part, 0] = high
        weigh[part, 1] = (turned - high.astype(F32)).astype(BF16)

    def product(left, right):
        return lax.dot_general(left, right, (((1,), (1,)), ((), ())), preferred_element_type=F32)

    def take(s):
        mine = arrived.at[s, x]
        landed(mine, recv_disp.at[s])
        remote(mine, mine, send_side.at[0], recv_side.at[s], e, across).start()

    def expand(s):
        acc = jnp.zeros((capacity, 4 * fpad), F32)
        for q in range(4):
            part = arrived[s, q // 2, :, (q % 2) * quarter:(q % 2 + 1) * quarter]
            acc = acc + product(part, gate_up[:, :, :, q * quarter:(q + 1) * quarter].reshape(4 * fpad, quarter))
        gate, up = acc[:, :2 * fpad], acc[:, 2 * fpad:]
        hidden[s, x] = (gate / (1.0 + jnp.exp(-gate)) * up).astype(BF16)
        remote(hidden.at[s, x], hidden.at[s, x], send_hid.at[0], recv_hid.at[s], e, across).start()

    def contract(s):
        landed(hidden.at[s, 1 - x], recv_hid.at[s])
        acc = jnp.zeros((capacity, half), F32)
        for side in range(2):
            acc = acc + jnp.dot(hidden[s, side], down_rows[side].reshape(2 * fpad, half), preferred_element_type=F32)
        for j in range(2):
            result[s, j] = acc[:, j * quarter:(j + 1) * quarter].astype(BF16)

    def home(s, r, peer, group):
        for j in range(2):
            remote(result.at[s, j], returned.at[r], send_home.at[0], recv_home.at[group], peer, 2 * x + j).start()

    def weights_ready():
        for kind in range(2):
            landed(owned(gate_up, kind, 1 - c), recv_weight.at[1 + kind])

    def relay_down():
        landed(far_rows, recv_weight.at[0])
        relay.start()

    def down_ready():
        landed(owned(down_rows, x, 1 - c), recv_weight.at[3])
        landed(owned(down_rows, 1 - x, 1 - c), recv_weight.at[4])

    def merge(part):
        back = returned[part * near:(part + 1) * near].reshape(slots // 2, quarter)
        return (jnp.dot(weigh[part, 0], back, preferred_element_type=F32)
                + jnp.dot(weigh[part, 1], back, preferred_element_type=F32))

    @pl.when(c == 1)
    def _():
        order = [(2 * step + odd, step, odd) for step in (outer, 1 - outer) for odd in range(2)]

        def far_take(i):
            take(order[i][0])

        def far_expand(i):
            s = order[i][0]
            landed(arrived.at[s, 1 - x], recv_side.at[s])
            expand(s)

        def far_contract(i):
            s, step, odd = order[i]
            contract(s)
            home(s, near + s, far_peer(step, odd), 2)

        far_take(0)
        far_take(1)
        weights_ready()
        relay_down()
        far_expand(0)
        far_take(2)
        far_expand(1)
        far_take(3)
        down_ready()
        far_contract(0)
        far_contract(1)
        far_expand(2)
        far_expand(3)
        far_contract(2)
        far_contract(3)
        landed(returned.at[0], recv_home.at[0])

    @pl.when(c == 0)
    def _():
        def near_expand(s):
            if s:
                landed(arrived.at[s], recv_disp.at[s])
            expand(s)

        def near_contract(s):
            contract(s)
            if s:
                home(s, s, toggled(e, s), 1)
            else:
                returned[0] = result[0, 0]
                remote(result.at[0, 1], returned.at[0], send_home.at[0], recv_home.at[0], e, partner).start()

        weights_ready()
        near_expand(0)
        near_expand(1)
        relay_down()
        down_ready()
        near_contract(0)
        near_contract(1)
        near_expand(3)
        near_expand(2)
        near_contract(3)
        near_contract(2)

    landed(returned.at[pl.ds(1, near - 1)], recv_home.at[1])
    total = merge(0)
    landed(returned.at[pl.ds(near, near)], recv_home.at[2])
    out_ref[...] = (total + merge(1)).astype(BF16)

    def finish():
        landed(hidden.at[:, x], send_hid.at[0])
        for share in shares:
            share.wait_send()
        relay.wait_send()

        @pl.when(c == 1)
        def _():
            landed(leaving, send_disp.at[0])
            landed(outgoing, send_disp.at[1])
            landed(arrived.at[:, x], send_side.at[0])
            landed(result, send_home.at[0])

        @pl.when(c == 0)
        def _():
            landed(outgoing.at[0], send_disp.at[0])
            landed(returned.at[pl.ds(0, 2 * near - 1)], send_home.at[0])

    finish()


def fused_body(tokens, norm_gain, routes, group_prob, expert_logits, gate_weight, up_weight, down_matrix):
    n_ep = lax.axis_size("ep")
    rows, model = tokens.shape
    capacity = 3 * routes.shape[1] * rows // (2 * n_ep)
    width = gate_weight.shape[2]
    fpad = round_up(width, 128)
    half, quarter = model // 2, model // 4
    sem = pltpu.SemaphoreType.DMA
    vmem = pl.BlockSpec(memory_space=pltpu.VMEM)
    operands = (
        tokens, norm_gain.reshape(1, model), routes.T, group_prob.reshape(1, rows), expert_logits.T,
        gate_weight.reshape(model, width).T, up_weight.reshape(model, width).T, down_matrix.reshape(width, model),
    )
    return pl.pallas_call(
        functools.partial(expert_kernel, n_ep, capacity, width),
        out_shape=jax.ShapeDtypeStruct((rows, quarter), BF16),
        in_specs=[pl.BlockSpec(memory_space=pl.ANY)] * 8,
        out_specs=vmem,
        scratch_shapes=[
            pltpu.VMEM((rows, model), BF16),
            pltpu.VMEM((1, model), F32),
            pltpu.VMEM((2, rows), jnp.int32),
            pltpu.VMEM((1, rows), F32),
            pltpu.VMEM((2, rows), F32),
            pltpu.VMEM((rows, model), BF16),
            pltpu.VMEM((n_ep * capacity, rows), BF16),
            pltpu.VMEM((2, 2, rows, n_ep * capacity // 2), BF16),
            pltpu.VMEM((n_ep // 2, capacity, half), BF16),
            pltpu.VMEM((2, 2, capacity, half), BF16),
            pltpu.VMEM((n_ep // 2, 2, capacity, half), BF16),
            pltpu.VMEM((2, 2, fpad, model), BF16),
            pltpu.VMEM((2, 2, fpad, half), BF16),
            pltpu.VMEM((width, half), BF16),
            pltpu.VMEM((n_ep // 2, 2, capacity, 2 * fpad), BF16),
            pltpu.VMEM((n_ep // 2, 2, capacity, quarter), BF16),
            pltpu.VMEM((n_ep, capacity, quarter), BF16),
            sem((9,)),
            sem((2,)), sem((n_ep // 2,)),
            sem((1,)), sem((n_ep // 2,)),
            sem((1,)), sem((n_ep // 2,)),
            sem((1,)), sem((3,)),
            sem((5,)), sem((5,)),
        ],
        compiler_params=pltpu.CompilerParams(
            collective_id=0, has_side_effects=True, vmem_limit_bytes=32 * 1024 * 1024),
    )(*[pltpu.with_memory_space_constraint(operand, pltpu.HBM) for operand in operands])


def fits_kernel(n_ep, n_tp, rows, experts, top, model):
    capacity = 3 * top * rows // (2 * experts)
    return (
        experts == n_ep and top == 2 and n_ep == 8 and n_tp == 4
        and capacity % 16 == 0 and rows % 128 == 0 and model % 512 == 0
    )


def solution(mesh):
    n_ep, n_tp = mesh.shape["ep"], mesh.shape["tp"]

    def chosen(*arrays):
        rows, model = arrays[0].shape
        fits = fits_kernel(n_ep, n_tp, rows, arrays[5].shape[0] * n_ep, arrays[2].shape[1], model)
        return (fused_body if fits else body)(*arrays)

    return jax.shard_map(
        chosen,
        mesh=mesh,
        in_specs=(
            P("ep", None),
            P(),
            P("ep", None),
            P("ep"),
            P("ep", None),
            P("ep", None, "tp"),
            P("ep", None, "tp"),
            P("ep", "tp", None),
        ),
        out_specs=P("ep", "tp"),
        check_vma=False,
    )
```

```python
import functools

import jax
import jax.numpy as jnp
from jax import lax
from jax.experimental import pallas as pl
from jax.experimental.pallas import tpu as pltpu
from jax.sharding import PartitionSpec as P


def hidden_part(buffer, gate_weight, up_weight):
    local_count = gate_weight.shape[0]
    grouped = buffer.reshape(
        buffer.shape[0] // local_count, local_count, buffer.shape[1], buffer.shape[2]
    )
    gate_proj = jnp.einsum(
        "sknd,kdf->sknf", grouped, gate_weight, preferred_element_type=jnp.float32
    )
    up_proj = jnp.einsum("sknd,kdf->sknf", grouped, up_weight, preferred_element_type=jnp.float32)
    hidden_state = (jax.nn.silu(gate_proj) * up_proj).astype(jnp.bfloat16)
    return hidden_state.reshape(buffer.shape[0], buffer.shape[1], hidden_state.shape[3])


def down_blocks(hidden_full, down_cols, block_count):
    local_count = down_cols.shape[0]
    width = hidden_full.shape[2] // block_count
    grouped = hidden_full.reshape(
        hidden_full.shape[0] // local_count, local_count, hidden_full.shape[1], block_count, width
    )
    columns = down_cols.reshape(local_count, block_count, width, down_cols.shape[2])
    block_list = jnp.einsum(
        "sknrf,krfd->sknrd", grouped, columns, preferred_element_type=jnp.float32
    ).astype(jnp.bfloat16)
    summed = jnp.sum(block_list.astype(jnp.float32), 3).astype(jnp.bfloat16)
    return summed.reshape(hidden_full.shape[0], hidden_full.shape[1], down_cols.shape[2])


def body(tokens, norm_gain, routes, group_prob, expert_logits, gate_weight, up_weight, down_matrix):
    tok_rows, model_width = tokens.shape
    top_count = routes.shape[1]
    experts = gate_weight.shape[0] * lax.axis_size("ep")
    capacity = 3 * top_count * tok_rows // (2 * experts)
    block_count = lax.axis_size("tp")
    down_cols = lax.all_to_all(down_matrix, "tp", split_axis=2, concat_axis=1, tiled=True)
    values = tokens.astype(jnp.float32)
    normed = (
        values * lax.rsqrt(jnp.mean(values * values, -1, keepdims=True) + 1e-06) * norm_gain
    ).astype(jnp.bfloat16)
    flat_ids = routes.reshape(-1)
    onehot = (flat_ids[:, None] == jnp.arange(experts, dtype=jnp.int32)[None, :]).astype(jnp.int32)
    earlier = jnp.cumsum(onehot, 0) - onehot
    slot_index = jnp.sum(earlier * onehot, 1)
    target = flat_ids * capacity + slot_index
    owners = jnp.arange(tok_rows * top_count, dtype=jnp.int32) // top_count
    outgoing = (
        jnp.zeros((experts * capacity, model_width), jnp.bfloat16).at[target].set(normed[owners])
    )
    outgoing = outgoing.reshape(experts, capacity, model_width)
    hidden_state = hidden_part(
        lax.all_to_all(outgoing, "ep", split_axis=0, concat_axis=0, tiled=True),
        gate_weight,
        up_weight,
    )
    hidden_full = lax.all_gather(hidden_state, "tp", axis=2, tiled=True)
    summed = down_blocks(hidden_full, down_cols, block_count)
    returned = lax.all_to_all(summed, "ep", split_axis=0, concat_axis=0, tiled=True)
    flat_back = returned.reshape(experts * capacity, returned.shape[2])
    weights = group_prob[:, None] * jax.nn.softmax(expert_logits, axis=-1)
    picked = flat_back[target].reshape(tok_rows, top_count, flat_back.shape[1]).astype(jnp.float32)
    combined = jnp.sum(picked * weights[:, :, None], 1).astype(jnp.bfloat16)
    return combined


MESH = pl.DeviceIdType.MESH
F32, BF16 = jnp.float32, jnp.bfloat16


def round_up(value, step):
    return -(-value // step) * step


def flipped(index, bit):
    return bit * (1 - 2 * ((index // bit) % 2))


def toggled(index, mask):
    result, bit = index, 1
    while bit <= mask:
        if mask & bit:
            result = result + flipped(index, bit)
        bit *= 2
    return result


def expert_kernel(
    n_ep, capacity, width,
    tokens_hbm, gain_hbm, routes_hbm, prob_hbm, logits_hbm, gate_ref, up_ref, down_ref,
    out_ref,
    tokens_ref, gain_ref, routes_ref, prob_ref, logits_ref, normed, select, weigh, leaving, spare, outgoing, arrived, gate_up,
    down_rows, down_other, hidden, result, returned,
    load_sem, send_disp, recv_disp, send_side, recv_side, send_hid, recv_hid, send_home, recv_home, send_weight, recv_weight,
):
    loads = [
        pltpu.make_async_copy(source, target, load_sem.at[i])
        for i, (source, target) in enumerate((
            (routes_hbm, routes_ref), (tokens_hbm, tokens_ref), (gain_hbm, gain_ref),
            (prob_hbm, prob_ref), (logits_hbm, logits_ref),
        ))
    ]
    for load in loads:
        load.start()
    rows, model = tokens_ref.shape
    half, quarter = model // 2, model // 4
    near = n_ep // 2
    slots = n_ep * capacity
    e = lax.axis_index("ep")
    t = lax.axis_index("tp")
    x, c = t // 2, t % 2
    partner, across = t + 1 - 2 * c, (t + 2) % 4
    outer = 1 - ((e // 2) % 2 + (e // 4) % 2) % 2

    hi, lo = e // 4, (e // 2) % 2

    barrier = pltpu.get_barrier_semaphore()
    for r in reversed(range(n_ep)):
        for mate in (t, partner):
            if r or mate is partner:
                pl.semaphore_signal(
                    barrier, inc=1, device_id={"ep": toggled(e, r), "tp": mate}, device_id_type=MESH)
    pl.semaphore_signal(barrier, inc=1, device_id={"ep": e, "tp": across}, device_id_type=MESH)

    def columns(side):
        return pl.ds(pl.multiple_of(side * half, half), half)

    def owned(ref, side, core):
        return ref.at[side, pl.ds(pl.multiple_of(core * width, width), width)]

    fetches = [
        pltpu.make_async_copy(down_ref.at[:, columns(1 - x)], down_other, load_sem.at[5]),
        pltpu.make_async_copy(gate_ref, owned(gate_up, 0, c), load_sem.at[6]),
        pltpu.make_async_copy(up_ref, owned(gate_up, 1, c), load_sem.at[7]),
        pltpu.make_async_copy(down_ref.at[:, columns(x)], owned(down_rows, x, c), load_sem.at[8]),
    ]
    for fetch in fetches:
        fetch.start()
    for load in loads:
        load.wait()

    first, second = routes_ref[0:1, :], routes_ref[1:2, :]
    lanes = round_up(n_ep, 16)
    expert_row = lax.broadcasted_iota(jnp.int32, (lanes, rows), 0)
    hit0 = (expert_row == first).astype(F32)
    hit1 = (expert_row == second).astype(F32)
    before = (
        lax.broadcasted_iota(jnp.int32, (rows, rows), 0) < lax.broadcasted_iota(jnp.int32, (rows, rows), 1)
    ).astype(F32).astype(BF16)
    earlier = jnp.dot((hit0 + hit1).astype(BF16), before, preferred_element_type=F32)
    slot0 = jnp.sum(earlier * hit0, 0, keepdims=True)
    slot1 = jnp.sum(earlier * hit1, 0, keepdims=True)
    place0 = (first ^ e) * capacity + slot0.astype(jnp.int32)
    place1 = (second ^ e) * capacity + slot1.astype(jnp.int32)
    slot_row = lax.broadcasted_iota(jnp.int32, (slots, rows), 0)
    at0, at1 = slot_row == place0, slot_row == place1
    select[...] = (at0.astype(F32) + at1.astype(F32)).astype(BF16)

    values = tokens_ref[...].astype(F32)
    scale = lax.rsqrt(jnp.mean(values * values, -1, keepdims=True) + 1e-06)
    normed[...] = (values * scale * gain_ref[...]).astype(BF16)

    def packed(begin, end, lanes):
        return jnp.dot(
            select[begin * capacity:end * capacity], normed[:, lanes], preferred_element_type=F32
        ).astype(BF16).reshape(end - begin, capacity, half)

    @pl.when(c == 1)
    def _():
        leaving[...] = packed(near, n_ep, columns(x))

    @pl.when(c == 0)
    def _():
        for side in range(2):
            both = packed(0, 2, slice(side * half, (side + 1) * half))
            arrived[0, side] = both[0]
            outgoing[0, side] = both[1]

    pl.semaphore_wait(barrier, 2 * n_ep)

    def remote(source, target, send, recv, ep, tp):
        return pltpu.make_async_remote_copy(
            src_ref=source, dst_ref=target, send_sem=send, recv_sem=recv,
            device_id={"ep": ep, "tp": tp}, device_id_type=MESH)

    def landed(ref, sem):
        pltpu.make_async_copy(ref, ref, sem).wait()

    def far_peer(step, odd):
        return e + flipped(e, 4) + step * flipped(e, 2) + odd * flipped(e, 1)

    def send_far(step):
        for odd in range(2):
            s = 2 * step + odd
            remote(leaving.at[s], arrived.at[s, x], send_disp.at[0], recv_disp.at[s], far_peer(step, odd), t).start()

    def pack_near():
        for side in range(2):
            outgoing[0:2, side] = packed(2, 4, slice(side * half, (side + 1) * half))

    first_step = outer

    @pl.when(c == 1)
    def _():
        send_far(first_step)
        send_far(1 - first_step)

        @pl.when(outer == 0)
        def _():
            spare[...] = packed(n_ep - 1, n_ep, columns(1 - x))[0]
            remote(spare, arrived.at[3, 1 - x], send_disp.at[2], recv_side.at[3], far_peer(1, 1), t).start()

    @pl.when(c == 1)
    def _():
        pack_near()

    @pl.when(c == 1)
    def _():
        for s in (3, 2):
            remote(outgoing.at[s - 2], arrived.at[s], send_disp.at[1], recv_disp.at[s], toggled(e, s), partner).start()

    @pl.when(c == 0)
    def _():
        remote(outgoing.at[0], arrived.at[1], send_disp.at[0], recv_disp.at[1], toggled(e, 1), t).start()

    shed = remote(down_other, owned(down_rows, x, c), send_weight.at[0], recv_weight.at[0], e, across)
    fetches[0].wait()
    shed.start()

    shares = [
        remote(owned(gate_up, 0, c), owned(gate_up, 0, c), send_weight.at[1], recv_weight.at[1], e, partner),
        remote(owned(gate_up, 1, c), owned(gate_up, 1, c), send_weight.at[2], recv_weight.at[2], e, partner),
        remote(owned(down_rows, x, c), owned(down_rows, x, c), send_weight.at[3], recv_weight.at[3], e, partner),
    ]
    for fetch, share in zip(fetches[1:], shares):
        fetch.wait()
        share.start()
    far_rows = owned(down_rows, 1 - x, c)
    relay = remote(far_rows, far_rows, send_weight.at[4], recv_weight.at[4], e, partner)

    logit0, logit1 = logits_ref[0:1, :], logits_ref[1:2, :]
    top = jnp.maximum(logit0, logit1)
    exp0, exp1 = jnp.exp(logit0 - top), jnp.exp(logit1 - top)
    share = prob_ref[...] / (exp0 + exp1)
    weight = jnp.where(at0, share * exp0, 0.0) + jnp.where(at1, share * exp1, 0.0)
    for part in range(2):
        turned = weight[part * (slots // 2):(part + 1) * (slots // 2)].T
        high = turned.astype(BF16)
        weigh[part, 0] = high
        weigh[part, 1] = (turned - high.astype(F32)).astype(BF16)

    def product(left, right):
        return lax.dot_general(left, right, (((1,), (1,)), ((), ())), preferred_element_type=F32)

    def take(s, on=True):
        mine = arrived.at[s, x]
        landed(mine, recv_disp.at[s])

        def pass_on():
            remote(mine, mine, send_side.at[0], recv_side.at[s], e, across).start()

        if on is True:
            pass_on()
        else:
            pl.when(on)(pass_on)

    def expand(s, begin=0, wait=None):
        gate = jnp.zeros((capacity, 2 * width), F32)
        up = jnp.zeros((capacity, 2 * width), F32)
        for side in (begin, 1 - begin):
            if wait is not None and side is not begin:
                wait()
            for q in range(2):
                part = arrived[s, side, :, q * quarter:(q + 1) * quarter]
                lanes = pl.ds(pl.multiple_of(side * half + q * quarter, quarter), quarter)
                gate = gate + product(part, gate_up[0, :, lanes])
                up = up + product(part, gate_up[1, :, lanes])
        hidden[s, x] = (gate / (1.0 + jnp.exp(-gate)) * up).astype(BF16)
        remote(hidden.at[s, x], hidden.at[s, x], send_hid.at[0], recv_hid.at[s], e, across).start()

    def contract(s):
        acc = jnp.dot(hidden[s, x], down_rows[x], preferred_element_type=F32)
        landed(hidden.at[s, 1 - x], recv_hid.at[s])
        acc = acc + jnp.dot(hidden[s, 1 - x], down_rows[1 - x], preferred_element_type=F32)
        for j in range(2):
            result[s, j] = acc[:, j * quarter:(j + 1) * quarter].astype(BF16)

    def home(s, r, peer, group):
        for j in range(2):
            remote(result.at[s, j], returned.at[r], send_home.at[0], recv_home.at[group], peer, 2 * x + j).start()

    def weights_ready():
        for kind in range(2):
            landed(owned(gate_up, kind, 1 - c), recv_weight.at[1 + kind])

    def relay_down():
        landed(far_rows, recv_weight.at[0])
        relay.start()

    def down_ready():
        landed(owned(down_rows, x, 1 - c), recv_weight.at[3])
        landed(owned(down_rows, 1 - x, 1 - c), recv_weight.at[4])

    def merge(part):
        back = returned[part * near:(part + 1) * near].reshape(slots // 2, quarter)
        return (jnp.dot(weigh[part, 0], back, preferred_element_type=F32)
                + jnp.dot(weigh[part, 1], back, preferred_element_type=F32))

    @pl.when(c == 1)
    def _():
        order = [
            (2 * step + odd, step, odd)
            for step, odd in ((outer, 0), (outer, 1), (1 - outer, 0), (1 - outer, 1))]

        def far_take(i):
            s, step, odd = order[i]
            take(s, (1 - outer) * step * odd == 0)

        def far_expand(i):
            s = order[i][0]
            expand(s, x, lambda: landed(arrived.at[s, 1 - x], recv_side.at[s]))

        def far_contract(i):
            s, step, odd = order[i]
            contract(s)
            home(s, near + s, far_peer(step, odd), 2)

        far_take(0)
        far_take(1)
        weights_ready()
        far_expand(0)
        far_take(2)
        far_expand(1)
        far_take(3)
        relay_down()
        down_ready()
        far_contract(0)
        far_expand(2)
        far_contract(1)
        far_expand(3)
        far_contract(2)
        far_contract(3)
        landed(returned.at[0], recv_home.at[0])

    @pl.when(c == 0)
    def _():
        def near_expand(s):
            if s:
                landed(arrived.at[s], recv_disp.at[s])
            expand(s)

        def near_contract(s):
            contract(s)
            if s:
                home(s, s, toggled(e, s), 1)
            else:
                returned[0] = result[0, 0]
                remote(result.at[0, 1], returned.at[0], send_home.at[0], recv_home.at[0], e, partner).start()

        weights_ready()
        near_expand(0)
        relay_down()
        near_expand(1)
        near_expand(3)
        near_expand(2)
        down_ready()
        near_contract(0)
        near_contract(1)
        near_contract(3)
        near_contract(2)

    landed(returned.at[pl.ds(1, near - 1)], recv_home.at[1])
    total = merge(0)
    landed(returned.at[pl.ds(near, near)], recv_home.at[2])
    out_ref[...] = (total + merge(1)).astype(BF16)

    def finish():
        landed(hidden.at[:, x], send_hid.at[0])
        shed.wait_send()
        for share in shares:
            share.wait_send()
        relay.wait_send()

        @pl.when(c == 1)
        def _():
            landed(leaving, send_disp.at[0])
            landed(outgoing, send_disp.at[1])

            @pl.when(outer == 0)
            def _():
                landed(spare, send_disp.at[2])
                landed(arrived.at[pl.ds(0, near - 1), x], send_side.at[0])

            @pl.when(outer == 1)
            def _():
                landed(arrived.at[:, x], send_side.at[0])

            landed(result, send_home.at[0])

        @pl.when(c == 0)
        def _():
            landed(outgoing.at[0], send_disp.at[0])
            landed(returned.at[pl.ds(0, 2 * near - 1)], send_home.at[0])

    finish()


def fused_body(tokens, norm_gain, routes, group_prob, expert_logits, gate_weight, up_weight, down_matrix):
    n_ep = lax.axis_size("ep")
    rows, model = tokens.shape
    capacity = 3 * routes.shape[1] * rows // (2 * n_ep)
    width = gate_weight.shape[2]
    half, quarter = model // 2, model // 4
    sem = pltpu.SemaphoreType.DMA
    vmem = pl.BlockSpec(memory_space=pltpu.VMEM)
    operands = (
        tokens, norm_gain.reshape(1, model), routes.T, group_prob.reshape(1, rows), expert_logits.T,
        gate_weight.reshape(model, width).T, up_weight.reshape(model, width).T, down_matrix.reshape(width, model),
    )
    return pl.pallas_call(
        functools.partial(expert_kernel, n_ep, capacity, width),
        out_shape=jax.ShapeDtypeStruct((rows, quarter), BF16),
        in_specs=[pl.BlockSpec(memory_space=pl.ANY)] * 8,
        out_specs=vmem,
        scratch_shapes=[
            pltpu.VMEM((rows, model), BF16),
            pltpu.VMEM((1, model), F32),
            pltpu.VMEM((2, rows), jnp.int32),
            pltpu.VMEM((1, rows), F32),
            pltpu.VMEM((2, rows), F32),
            pltpu.VMEM((rows, model), BF16),
            pltpu.VMEM((n_ep * capacity, rows), BF16),
            pltpu.VMEM((2, 2, rows, n_ep * capacity // 2), BF16),
            pltpu.VMEM((n_ep // 2, capacity, half), BF16),
            pltpu.VMEM((capacity, half), BF16),
            pltpu.VMEM((2, 2, capacity, half), BF16),
            pltpu.VMEM((n_ep // 2, 2, capacity, half), BF16),
            pltpu.VMEM((2, 2 * width, model), BF16),
            pltpu.VMEM((2, 2 * width, half), BF16),
            pltpu.VMEM((width, half), BF16),
            pltpu.VMEM((n_ep // 2, 2, capacity, 2 * width), BF16),
            pltpu.VMEM((n_ep // 2, 2, capacity, quarter), BF16),
            pltpu.VMEM((n_ep, capacity, quarter), BF16),
            sem((9,)),
            sem((3,)), sem((n_ep // 2,)),
            sem((1,)), sem((n_ep // 2,)),
            sem((1,)), sem((n_ep // 2,)),
            sem((1,)), sem((3,)),
            sem((5,)), sem((5,)),
        ],
        compiler_params=pltpu.CompilerParams(
            collective_id=0, has_side_effects=True, vmem_limit_bytes=32 * 1024 * 1024),
    )(*[pltpu.with_memory_space_constraint(operand, pltpu.HBM) for operand in operands])


def fits_kernel(n_ep, n_tp, rows, experts, top, model, width):
    capacity = 3 * top * rows // (2 * experts)
    return (
        experts == n_ep and top == 2 and n_ep == 8 and n_tp == 4
        and capacity % 16 == 0 and rows % 128 == 0 and model % 512 == 0 and width % 16 == 0
    )


def solution(mesh):
    n_ep, n_tp = mesh.shape["ep"], mesh.shape["tp"]

    def chosen(*arrays):
        rows, model = arrays[0].shape
        fits = fits_kernel(n_ep, n_tp, rows, arrays[5].shape[0] * n_ep, arrays[2].shape[1], model, arrays[5].shape[2])
        return (fused_body if fits else body)(*arrays)

    return jax.shard_map(
        chosen,
        mesh=mesh,
        in_specs=(
            P("ep", None),
            P(),
            P("ep", None),
            P("ep"),
            P("ep", None),
            P("ep", None, "tp"),
            P("ep", None, "tp"),
            P("ep", "tp", None),
        ),
        out_specs=P("ep", "tp"),
        check_vma=False,
    )
```

```python
import functools

import jax
import jax.numpy as jnp
from jax import lax
from jax.experimental import pallas as pl
from jax.experimental.pallas import tpu as pltpu
from jax.sharding import PartitionSpec as P


def hidden_part(buffer, gate_weight, up_weight):
    local_count = gate_weight.shape[0]
    grouped = buffer.reshape(
        buffer.shape[0] // local_count, local_count, buffer.shape[1], buffer.shape[2]
    )
    gate_proj = jnp.einsum(
        "sknd,kdf->sknf", grouped, gate_weight, preferred_element_type=jnp.float32
    )
    up_proj = jnp.einsum("sknd,kdf->sknf", grouped, up_weight, preferred_element_type=jnp.float32)
    hidden_state = (jax.nn.silu(gate_proj) * up_proj).astype(jnp.bfloat16)
    return hidden_state.reshape(buffer.shape[0], buffer.shape[1], hidden_state.shape[3])


def down_blocks(hidden_full, down_cols, block_count):
    local_count = down_cols.shape[0]
    width = hidden_full.shape[2] // block_count
    grouped = hidden_full.reshape(
        hidden_full.shape[0] // local_count, local_count, hidden_full.shape[1], block_count, width
    )
    columns = down_cols.reshape(local_count, block_count, width, down_cols.shape[2])
    block_list = jnp.einsum(
        "sknrf,krfd->sknrd", grouped, columns, preferred_element_type=jnp.float32
    ).astype(jnp.bfloat16)
    summed = jnp.sum(block_list.astype(jnp.float32), 3).astype(jnp.bfloat16)
    return summed.reshape(hidden_full.shape[0], hidden_full.shape[1], down_cols.shape[2])


def body(tokens, norm_gain, routes, group_prob, expert_logits, gate_weight, up_weight, down_matrix):
    tok_rows, model_width = tokens.shape
    top_count = routes.shape[1]
    experts = gate_weight.shape[0] * lax.axis_size("ep")
    capacity = 3 * top_count * tok_rows // (2 * experts)
    block_count = lax.axis_size("tp")
    down_cols = lax.all_to_all(down_matrix, "tp", split_axis=2, concat_axis=1, tiled=True)
    values = tokens.astype(jnp.float32)
    normed = (
        values * lax.rsqrt(jnp.mean(values * values, -1, keepdims=True) + 1e-06) * norm_gain
    ).astype(jnp.bfloat16)
    flat_ids = routes.reshape(-1)
    onehot = (flat_ids[:, None] == jnp.arange(experts, dtype=jnp.int32)[None, :]).astype(jnp.int32)
    earlier = jnp.cumsum(onehot, 0) - onehot
    slot_index = jnp.sum(earlier * onehot, 1)
    target = flat_ids * capacity + slot_index
    owners = jnp.arange(tok_rows * top_count, dtype=jnp.int32) // top_count
    outgoing = (
        jnp.zeros((experts * capacity, model_width), jnp.bfloat16).at[target].set(normed[owners])
    )
    outgoing = outgoing.reshape(experts, capacity, model_width)
    hidden_state = hidden_part(
        lax.all_to_all(outgoing, "ep", split_axis=0, concat_axis=0, tiled=True),
        gate_weight,
        up_weight,
    )
    hidden_full = lax.all_gather(hidden_state, "tp", axis=2, tiled=True)
    summed = down_blocks(hidden_full, down_cols, block_count)
    returned = lax.all_to_all(summed, "ep", split_axis=0, concat_axis=0, tiled=True)
    flat_back = returned.reshape(experts * capacity, returned.shape[2])
    weights = group_prob[:, None] * jax.nn.softmax(expert_logits, axis=-1)
    picked = flat_back[target].reshape(tok_rows, top_count, flat_back.shape[1]).astype(jnp.float32)
    combined = jnp.sum(picked * weights[:, :, None], 1).astype(jnp.bfloat16)
    return combined


MESH = pl.DeviceIdType.MESH
F32, BF16 = jnp.float32, jnp.bfloat16


def round_up(value, step):
    return -(-value // step) * step


def flipped(index, bit):
    return bit * (1 - 2 * ((index // bit) % 2))


def toggled(index, mask):
    result, bit = index, 1
    while bit <= mask:
        if mask & bit:
            result = result + flipped(index, bit)
        bit *= 2
    return result


def expert_kernel(
    n_ep, capacity, width,
    tokens_hbm, gain_hbm, routes_hbm, prob_hbm, logits_hbm, gate_ref, up_ref, down_ref,
    out_ref,
    tokens_ref, gain_ref, routes_ref, prob_ref, logits_ref, normed, select, weigh, leaving, spare, outgoing, arrived, gate_up,
    down_rows, down_other, hidden, result, returned,
    load_sem, send_disp, recv_disp, send_side, recv_side, send_hid, recv_hid, send_home, recv_home, send_weight, recv_weight, ready,
):
    loads = [
        pltpu.make_async_copy(source, target, load_sem.at[i])
        for i, (source, target) in enumerate((
            (routes_hbm, routes_ref), (tokens_hbm, tokens_ref), (gain_hbm, gain_ref),
            (prob_hbm, prob_ref), (logits_hbm, logits_ref),
        ))
    ]
    for load in loads:
        load.start()
    rows, model = tokens_ref.shape
    half, quarter = model // 2, model // 4
    near = n_ep // 2
    slots = n_ep * capacity
    e = lax.axis_index("ep")
    t = lax.axis_index("tp")
    x, c = t // 2, t % 2
    partner, across = t + 1 - 2 * c, (t + 2) % 4
    outer = 1 - ((e // 2) % 2 + (e // 4) % 2) % 2

    hi, lo = e // 4, (e // 2) % 2

    barrier = pltpu.get_barrier_semaphore()

    def greet(semaphore, ep, tp):
        pl.semaphore_signal(semaphore, inc=1, device_id={"ep": ep, "tp": tp}, device_id_type=MESH)

    for r in reversed(range(1, n_ep)):
        greet(barrier, toggled(e, r), t)
    greet(barrier, e, across)

    @pl.when(c == 1)
    def _():
        for r in reversed(range(n_ep)):
            greet(barrier, toggled(e, r), partner)

    def columns(side):
        return pl.ds(pl.multiple_of(side * half, half), half)

    def owned(ref, side, core):
        return ref.at[side, pl.ds(pl.multiple_of(core * width, width), width)]

    fetches = [
        pltpu.make_async_copy(down_ref.at[:, columns(1 - x)], down_other, load_sem.at[5]),
        pltpu.make_async_copy(gate_ref, owned(gate_up, 0, c), load_sem.at[6]),
        pltpu.make_async_copy(up_ref, owned(gate_up, 1, c), load_sem.at[7]),
        pltpu.make_async_copy(down_ref.at[:, columns(x)], owned(down_rows, x, c), load_sem.at[8]),
    ]
    for fetch in fetches:
        fetch.start()
    for load in loads:
        load.wait()

    first, second = routes_ref[0:1, :], routes_ref[1:2, :]
    lanes = round_up(n_ep, 16)
    expert_row = lax.broadcasted_iota(jnp.int32, (lanes, rows), 0)
    hit0 = (expert_row == first).astype(F32)
    hit1 = (expert_row == second).astype(F32)
    before = (
        lax.broadcasted_iota(jnp.int32, (rows, rows), 0) < lax.broadcasted_iota(jnp.int32, (rows, rows), 1)
    ).astype(F32).astype(BF16)
    earlier = jnp.dot((hit0 + hit1).astype(BF16), before, preferred_element_type=F32)
    slot0 = jnp.sum(earlier * hit0, 0, keepdims=True)
    slot1 = jnp.sum(earlier * hit1, 0, keepdims=True)
    place0 = (first ^ e) * capacity + slot0.astype(jnp.int32)
    place1 = (second ^ e) * capacity + slot1.astype(jnp.int32)
    slot_row = lax.broadcasted_iota(jnp.int32, (slots, rows), 0)
    at0, at1 = slot_row == place0, slot_row == place1
    select[...] = (at0.astype(F32) + at1.astype(F32)).astype(BF16)

    values = tokens_ref[...].astype(F32)
    scale = lax.rsqrt(jnp.mean(values * values, -1, keepdims=True) + 1e-06)
    normed[...] = (values * scale * gain_ref[...]).astype(BF16)

    def packed(begin, end, q):
        lanes = pl.ds(pl.multiple_of(q * quarter, quarter), quarter)
        return jnp.dot(
            select[begin * capacity:end * capacity], normed[:, lanes], preferred_element_type=F32
        ).astype(BF16).reshape(end - begin, capacity, quarter)

    @pl.when(c == 1)
    def _():
        for q in range(2):
            leaving[:, q] = packed(near, n_ep, 2 * x + q)

    @pl.when(c == 0)
    def _():
        for q in range(4):
            both = packed(0, 2, q)
            arrived[0, q] = both[0]
            outgoing[0, q] = both[1]

    @pl.when(c == 1)
    def _():
        pl.semaphore_wait(barrier, n_ep)

    @pl.when(c == 0)
    def _():
        pl.semaphore_wait(barrier, 2 * n_ep)
        greet(ready, e, partner)

    def remote(source, target, send, recv, ep, tp):
        return pltpu.make_async_remote_copy(
            src_ref=source, dst_ref=target, send_sem=send, recv_sem=recv,
            device_id={"ep": ep, "tp": tp}, device_id_type=MESH)

    def landed(ref, sem):
        pltpu.make_async_copy(ref, ref, sem).wait()

    own_half, their_half = pl.ds(2 * x, 2), pl.ds(2 - 2 * x, 2)

    def far_peer(step, odd):
        return e + flipped(e, 4) + step * flipped(e, 2) + odd * flipped(e, 1)

    def send_far(step):
        for odd in range(2):
            s = 2 * step + odd
            for q in range(2):
                remote(
                    leaving.at[s, q], arrived.at[s, 2 * x + q], send_disp.at[0], recv_disp.at[near * q + s],
                    far_peer(step, odd), t).start()

    def pack_near():
        for q in range(4):
            outgoing[0:2, q] = packed(2, 4, q)

    first_step = outer

    @pl.when(c == 1)
    def _():
        send_far(first_step)
        send_far(1 - first_step)

    @pl.when(c == 1)
    def _():
        pack_near()

    @pl.when(c == 1)
    def _():
        pl.semaphore_wait(ready, 1)

    def send_near(s):
        remote(outgoing.at[s - 2], arrived.at[s], send_disp.at[1], recv_disp.at[s], toggled(e, s), partner).start()

    @pl.when(c == 1)
    def _():

        @pl.when(outer == 0)
        def _():
            send_near(3)
            send_near(2)

    @pl.when(c == 0)
    def _():
        remote(outgoing.at[0], arrived.at[1], send_disp.at[0], recv_disp.at[1], toggled(e, 1), t).start()

    shed = remote(down_other, owned(down_rows, x, c), send_weight.at[0], recv_weight.at[0], e, across)
    fetches[0].wait()
    shed.start()

    shares = [
        remote(owned(gate_up, 0, c), owned(gate_up, 0, c), send_weight.at[1], recv_weight.at[1], e, partner),
        remote(owned(gate_up, 1, c), owned(gate_up, 1, c), send_weight.at[2], recv_weight.at[2], e, partner),
        remote(owned(down_rows, x, c), owned(down_rows, x, c), send_weight.at[3], recv_weight.at[3], e, partner),
    ]
    for fetch, share in zip(fetches[1:], shares):
        fetch.wait()
        share.start()
    far_rows = owned(down_rows, 1 - x, c)
    relay = remote(far_rows, far_rows, send_weight.at[4], recv_weight.at[4], e, partner)

    logit0, logit1 = logits_ref[0:1, :], logits_ref[1:2, :]
    top = jnp.maximum(logit0, logit1)
    exp0, exp1 = jnp.exp(logit0 - top), jnp.exp(logit1 - top)
    share = prob_ref[...] / (exp0 + exp1)
    weight = jnp.where(at0, share * exp0, 0.0) + jnp.where(at1, share * exp1, 0.0)
    for part in range(2):
        turned = weight[part * (slots // 2):(part + 1) * (slots // 2)].T
        high = turned.astype(BF16)
        weigh[part, 0] = high
        weigh[part, 1] = (turned - high.astype(F32)).astype(BF16)

    def product(left, right):
        return lax.dot_general(left, right, (((1,), (1,)), ((), ())), preferred_element_type=F32)

    def take(s, on=True):
        for q in range(2):
            mine = arrived.at[s, 2 * x + q]
            landed(mine, recv_disp.at[near * q + s])

            @pl.when(on)
            def _():
                remote(mine, mine, send_side.at[0], recv_side.at[s], e, across).start()

    def expand(s, begin=0, wait=None):
        gate = jnp.zeros((capacity, 2 * width), F32)
        up = jnp.zeros((capacity, 2 * width), F32)
        for side in (begin, 1 - begin):
            if wait is not None and side is not begin:
                wait()
            for q in range(2):
                part = arrived[s, 2 * side + q]
                lanes = pl.ds(pl.multiple_of(side * half + q * quarter, quarter), quarter)
                gate = gate + product(part, gate_up[0, :, lanes])
                up = up + product(part, gate_up[1, :, lanes])
        hidden[s, x] = (gate / (1.0 + jnp.exp(-gate)) * up).astype(BF16)
        remote(hidden.at[s, x], hidden.at[s, x], send_hid.at[0], recv_hid.at[s], e, across).start()

    def contract(s):
        acc = jnp.dot(hidden[s, x], down_rows[x], preferred_element_type=F32)
        landed(hidden.at[s, 1 - x], recv_hid.at[s])
        acc = acc + jnp.dot(hidden[s, 1 - x], down_rows[1 - x], preferred_element_type=F32)
        for j in range(2):
            result[s, j] = acc[:, j * quarter:(j + 1) * quarter].astype(BF16)

    def home(s, r, peer, group):
        for j in range(2):
            remote(result.at[s, j], returned.at[r], send_home.at[0], recv_home.at[group], peer, 2 * x + j).start()

    def weights_ready():
        for kind in range(2):
            landed(owned(gate_up, kind, 1 - c), recv_weight.at[1 + kind])

    def relay_down():
        landed(far_rows, recv_weight.at[0])
        relay.start()

    def down_ready():
        landed(owned(down_rows, x, 1 - c), recv_weight.at[3])
        landed(owned(down_rows, 1 - x, 1 - c), recv_weight.at[4])

    def merge(part):
        back = returned[part * near:(part + 1) * near].reshape(slots // 2, quarter)
        return (jnp.dot(weigh[part, 0], back, preferred_element_type=F32)
                + jnp.dot(weigh[part, 1], back, preferred_element_type=F32))

    @pl.when(c == 1)
    def _():
        order = [
            (2 * step + odd, step, odd)
            for step, odd in ((outer, 0), (outer, 1), (1 - outer, 0), (1 - outer, 1))]

        def far_take(i):
            s, step, odd = order[i]
            take(s)

        def far_expand(i):
            s = order[i][0]
            expand(s, x, lambda: landed(arrived.at[s, their_half], recv_side.at[s]))

        def far_contract(i):
            s, step, odd = order[i]
            contract(s)
            home(s, near + s, far_peer(step, odd), 2)

        far_take(0)
        far_take(1)

        @pl.when(outer == 1)
        def _():
            send_near(3)
            send_near(2)

        weights_ready()
        far_expand(0)
        far_take(2)
        far_expand(1)
        far_take(3)
        relay_down()
        down_ready()
        far_contract(0)
        far_expand(2)
        far_contract(1)
        far_expand(3)
        far_contract(2)
        far_contract(3)
        landed(returned.at[0], recv_home.at[0])

    @pl.when(c == 0)
    def _():
        def near_expand(s):
            if s:
                landed(arrived.at[s], recv_disp.at[s])
            expand(s)

        def near_contract(s):
            contract(s)
            if s:
                home(s, s, toggled(e, s), 1)
            else:
                returned[0] = result[0, 0]
                remote(result.at[0, 1], returned.at[0], send_home.at[0], recv_home.at[0], e, partner).start()

        weights_ready()
        near_expand(0)
        relay_down()
        near_expand(1)
        near_expand(3)
        near_expand(2)
        down_ready()
        near_contract(0)
        near_contract(1)
        near_contract(3)
        near_contract(2)

    landed(returned.at[pl.ds(1, near - 1)], recv_home.at[1])
    total = merge(0)
    landed(returned.at[pl.ds(near, near)], recv_home.at[2])
    out_ref[...] = (total + merge(1)).astype(BF16)

    def finish():
        landed(hidden.at[:, x], send_hid.at[0])
        shed.wait_send()
        for share in shares:
            share.wait_send()
        relay.wait_send()

        @pl.when(c == 1)
        def _():
            landed(leaving, send_disp.at[0])
            landed(outgoing, send_disp.at[1])

            landed(arrived.at[:, own_half], send_side.at[0])
            landed(result, send_home.at[0])

        @pl.when(c == 0)
        def _():
            landed(outgoing.at[0], send_disp.at[0])
            landed(returned.at[pl.ds(0, 2 * near - 1)], send_home.at[0])

    finish()


def fused_body(tokens, norm_gain, routes, group_prob, expert_logits, gate_weight, up_weight, down_matrix):
    n_ep = lax.axis_size("ep")
    rows, model = tokens.shape
    capacity = 3 * routes.shape[1] * rows // (2 * n_ep)
    width = gate_weight.shape[2]
    half, quarter = model // 2, model // 4
    sem = pltpu.SemaphoreType.DMA
    vmem = pl.BlockSpec(memory_space=pltpu.VMEM)
    operands = (
        tokens, norm_gain.reshape(1, model), routes.T, group_prob.reshape(1, rows), expert_logits.T,
        gate_weight.reshape(model, width).T, up_weight.reshape(model, width).T, down_matrix.reshape(width, model),
    )
    return pl.pallas_call(
        functools.partial(expert_kernel, n_ep, capacity, width),
        out_shape=jax.ShapeDtypeStruct((rows, quarter), BF16),
        in_specs=[pl.BlockSpec(memory_space=pl.ANY)] * 8,
        out_specs=vmem,
        scratch_shapes=[
            pltpu.VMEM((rows, model), BF16),
            pltpu.VMEM((1, model), F32),
            pltpu.VMEM((2, rows), jnp.int32),
            pltpu.VMEM((1, rows), F32),
            pltpu.VMEM((2, rows), F32),
            pltpu.VMEM((rows, model), BF16),
            pltpu.VMEM((n_ep * capacity, rows), BF16),
            pltpu.VMEM((2, 2, rows, n_ep * capacity // 2), BF16),
            pltpu.VMEM((n_ep // 2, 2, capacity, quarter), BF16),
            pltpu.VMEM((2, capacity, quarter), BF16),
            pltpu.VMEM((2, 4, capacity, quarter), BF16),
            pltpu.VMEM((n_ep // 2, 4, capacity, quarter), BF16),
            pltpu.VMEM((2, 2 * width, model), BF16),
            pltpu.VMEM((2, 2 * width, half), BF16),
            pltpu.VMEM((width, half), BF16),
            pltpu.VMEM((n_ep // 2, 2, capacity, 2 * width), BF16),
            pltpu.VMEM((n_ep // 2, 2, capacity, quarter), BF16),
            pltpu.VMEM((n_ep, capacity, quarter), BF16),
            sem((9,)),
            sem((2,)), sem((n_ep,)),
            sem((1,)), sem((n_ep // 2,)),
            sem((1,)), sem((n_ep // 2,)),
            sem((1,)), sem((3,)),
            sem((5,)), sem((5,)), pltpu.SemaphoreType.REGULAR,
        ],
        compiler_params=pltpu.CompilerParams(
            collective_id=0, has_side_effects=True, vmem_limit_bytes=32 * 1024 * 1024),
    )(*[pltpu.with_memory_space_constraint(operand, pltpu.HBM) for operand in operands])


def fits_kernel(n_ep, n_tp, rows, experts, top, model, width):
    capacity = 3 * top * rows // (2 * experts)
    return (
        experts == n_ep and top == 2 and n_ep == 8 and n_tp == 4
        and capacity % 16 == 0 and rows % 128 == 0 and model % 512 == 0 and width % 16 == 0
    )


def solution(mesh):
    n_ep, n_tp = mesh.shape["ep"], mesh.shape["tp"]

    def chosen(*arrays):
        rows, model = arrays[0].shape
        fits = fits_kernel(n_ep, n_tp, rows, arrays[5].shape[0] * n_ep, arrays[2].shape[1], model, arrays[5].shape[2])
        return (fused_body if fits else body)(*arrays)

    return jax.shard_map(
        chosen,
        mesh=mesh,
        in_specs=(
            P("ep", None),
            P(),
            P("ep", None),
            P("ep"),
            P("ep", None),
            P("ep", None, "tp"),
            P("ep", None, "tp"),
            P("ep", "tp", None),
        ),
        out_specs=P("ep", "tp"),
        check_vma=False,
    )
```

```python
import functools

import jax
import jax.numpy as jnp
from jax import lax
from jax.experimental import pallas as pl
from jax.experimental.pallas import tpu as pltpu
from jax.sharding import PartitionSpec as P


def hidden_part(buffer, gate_weight, up_weight):
    local_count = gate_weight.shape[0]
    grouped = buffer.reshape(
        buffer.shape[0] // local_count, local_count, buffer.shape[1], buffer.shape[2]
    )
    gate_proj = jnp.einsum(
        "sknd,kdf->sknf", grouped, gate_weight, preferred_element_type=jnp.float32
    )
    up_proj = jnp.einsum("sknd,kdf->sknf", grouped, up_weight, preferred_element_type=jnp.float32)
    hidden_state = (jax.nn.silu(gate_proj) * up_proj).astype(jnp.bfloat16)
    return hidden_state.reshape(buffer.shape[0], buffer.shape[1], hidden_state.shape[3])


def down_blocks(hidden_full, down_cols, block_count):
    local_count = down_cols.shape[0]
    width = hidden_full.shape[2] // block_count
    grouped = hidden_full.reshape(
        hidden_full.shape[0] // local_count, local_count, hidden_full.shape[1], block_count, width
    )
    columns = down_cols.reshape(local_count, block_count, width, down_cols.shape[2])
    block_list = jnp.einsum(
        "sknrf,krfd->sknrd", grouped, columns, preferred_element_type=jnp.float32
    ).astype(jnp.bfloat16)
    summed = jnp.sum(block_list.astype(jnp.float32), 3).astype(jnp.bfloat16)
    return summed.reshape(hidden_full.shape[0], hidden_full.shape[1], down_cols.shape[2])


def body(tokens, norm_gain, routes, group_prob, expert_logits, gate_weight, up_weight, down_matrix):
    tok_rows, model_width = tokens.shape
    top_count = routes.shape[1]
    experts = gate_weight.shape[0] * lax.axis_size("ep")
    capacity = 3 * top_count * tok_rows // (2 * experts)
    block_count = lax.axis_size("tp")
    down_cols = lax.all_to_all(down_matrix, "tp", split_axis=2, concat_axis=1, tiled=True)
    values = tokens.astype(jnp.float32)
    normed = (
        values * lax.rsqrt(jnp.mean(values * values, -1, keepdims=True) + 1e-06) * norm_gain
    ).astype(jnp.bfloat16)
    flat_ids = routes.reshape(-1)
    onehot = (flat_ids[:, None] == jnp.arange(experts, dtype=jnp.int32)[None, :]).astype(jnp.int32)
    earlier = jnp.cumsum(onehot, 0) - onehot
    slot_index = jnp.sum(earlier * onehot, 1)
    target = flat_ids * capacity + slot_index
    owners = jnp.arange(tok_rows * top_count, dtype=jnp.int32) // top_count
    outgoing = (
        jnp.zeros((experts * capacity, model_width), jnp.bfloat16).at[target].set(normed[owners])
    )
    outgoing = outgoing.reshape(experts, capacity, model_width)
    hidden_state = hidden_part(
        lax.all_to_all(outgoing, "ep", split_axis=0, concat_axis=0, tiled=True),
        gate_weight,
        up_weight,
    )
    hidden_full = lax.all_gather(hidden_state, "tp", axis=2, tiled=True)
    summed = down_blocks(hidden_full, down_cols, block_count)
    returned = lax.all_to_all(summed, "ep", split_axis=0, concat_axis=0, tiled=True)
    flat_back = returned.reshape(experts * capacity, returned.shape[2])
    weights = group_prob[:, None] * jax.nn.softmax(expert_logits, axis=-1)
    picked = flat_back[target].reshape(tok_rows, top_count, flat_back.shape[1]).astype(jnp.float32)
    combined = jnp.sum(picked * weights[:, :, None], 1).astype(jnp.bfloat16)
    return combined


MESH = pl.DeviceIdType.MESH
F32, BF16 = jnp.float32, jnp.bfloat16


def round_up(value, step):
    return -(-value // step) * step


def flipped(index, bit):
    return bit * (1 - 2 * ((index // bit) % 2))


def toggled(index, mask):
    result, bit = index, 1
    while bit <= mask:
        if mask & bit:
            result = result + flipped(index, bit)
        bit *= 2
    return result


def expert_kernel(
    n_ep, capacity, width,
    tokens_hbm, gain_hbm, routes_hbm, prob_hbm, logits_hbm, gate_ref, up_ref, down_ref,
    out_ref,
    tokens_ref, gain_ref, routes_ref, prob_ref, logits_ref, normed, select, weigh, leaving, spare, outgoing, arrived, gate_up,
    down_rows, down_other, hidden, result, returned,
    load_sem, send_disp, recv_disp, send_side, recv_side, send_hid, recv_hid, send_home, recv_home, send_weight, recv_weight, ready,
):
    loads = [
        pltpu.make_async_copy(source, target, load_sem.at[i])
        for i, (source, target) in enumerate((
            (routes_hbm, routes_ref), (tokens_hbm, tokens_ref), (gain_hbm, gain_ref),
            (prob_hbm, prob_ref), (logits_hbm, logits_ref),
        ))
    ]
    for load in loads:
        load.start()
    rows, model = tokens_ref.shape
    half, quarter = model // 2, model // 4
    near = n_ep // 2
    slots = n_ep * capacity
    e = lax.axis_index("ep")
    t = lax.axis_index("tp")
    x, c = t // 2, t % 2
    partner, across = t + 1 - 2 * c, (t + 2) % 4
    outer = 1 - ((e // 2) % 2 + (e // 4) % 2) % 2

    hi, lo = e // 4, (e // 2) % 2

    barrier = pltpu.get_barrier_semaphore()

    def greet(semaphore, ep, tp):
        pl.semaphore_signal(semaphore, inc=1, device_id={"ep": ep, "tp": tp}, device_id_type=MESH)

    for r in reversed(range(1, n_ep)):
        greet(barrier, toggled(e, r), t)
    greet(barrier, e, across)

    @pl.when(c == 1)
    def _():
        for r in reversed(range(n_ep)):
            greet(barrier, toggled(e, r), partner)

    def columns(side):
        return pl.ds(pl.multiple_of(side * half, half), half)

    def owned(ref, side, core):
        return ref.at[side, pl.ds(pl.multiple_of(core * width, width), width)]

    fetches = [
        pltpu.make_async_copy(down_ref.at[:, columns(1 - x)], down_other, load_sem.at[5]),
        pltpu.make_async_copy(gate_ref, owned(gate_up, 0, c), load_sem.at[6]),
        pltpu.make_async_copy(up_ref, owned(gate_up, 1, c), load_sem.at[7]),
        pltpu.make_async_copy(down_ref.at[:, columns(x)], owned(down_rows, x, c), load_sem.at[8]),
    ]
    for fetch in fetches:
        fetch.start()
    for load in loads:
        load.wait()

    first, second = routes_ref[0:1, :], routes_ref[1:2, :]
    lanes = round_up(n_ep, 16)
    expert_row = lax.broadcasted_iota(jnp.int32, (lanes, rows), 0)
    hit0 = (expert_row == first).astype(F32)
    hit1 = (expert_row == second).astype(F32)
    before = (
        lax.broadcasted_iota(jnp.int32, (rows, rows), 0) < lax.broadcasted_iota(jnp.int32, (rows, rows), 1)
    ).astype(F32).astype(BF16)
    earlier = jnp.dot((hit0 + hit1).astype(BF16), before, preferred_element_type=F32)
    slot0 = jnp.sum(earlier * hit0, 0, keepdims=True)
    slot1 = jnp.sum(earlier * hit1, 0, keepdims=True)
    place0 = (first ^ e) * capacity + slot0.astype(jnp.int32)
    place1 = (second ^ e) * capacity + slot1.astype(jnp.int32)
    slot_row = lax.broadcasted_iota(jnp.int32, (slots, rows), 0)
    at0, at1 = slot_row == place0, slot_row == place1
    select[...] = (at0.astype(F32) + at1.astype(F32)).astype(BF16)

    values = tokens_ref[...].astype(F32)
    scale = lax.rsqrt(jnp.mean(values * values, -1, keepdims=True) + 1e-06)
    normed[...] = (values * scale * gain_ref[...]).astype(BF16)

    def packed(begin, end, q):
        lanes = pl.ds(pl.multiple_of(q * quarter, quarter), quarter)
        return jnp.dot(
            select[begin * capacity:end * capacity], normed[:, lanes], preferred_element_type=F32
        ).astype(BF16).reshape(end - begin, capacity, quarter)

    @pl.when(c == 1)
    def _():
        for q in range(2):
            leaving[:, q] = packed(near, n_ep, 2 * x + q)

    @pl.when(c == 0)
    def _():
        for q in range(4):
            both = packed(0, 2, q)
            arrived[0, q] = both[0]
            outgoing[0, q] = both[1]

    @pl.when(c == 1)
    def _():
        pl.semaphore_wait(barrier, n_ep)

    @pl.when(c == 0)
    def _():
        pl.semaphore_wait(barrier, 2 * n_ep)
        greet(ready, e, partner)

    def remote(source, target, send, recv, ep, tp):
        return pltpu.make_async_remote_copy(
            src_ref=source, dst_ref=target, send_sem=send, recv_sem=recv,
            device_id={"ep": ep, "tp": tp}, device_id_type=MESH)

    def landed(ref, sem):
        pltpu.make_async_copy(ref, ref, sem).wait()

    own_half, their_half = pl.ds(2 * x, 2), pl.ds(2 - 2 * x, 2)

    def far_peer(step, odd):
        return e + flipped(e, 4) + step * flipped(e, 2) + odd * flipped(e, 1)

    def send_far(step):
        for odd in range(2):
            s = 2 * step + odd
            for q in range(2):
                remote(
                    leaving.at[s, q], arrived.at[s, 2 * x + q], send_disp.at[0], recv_disp.at[near * q + s],
                    far_peer(step, odd), t).start()

    def pack_near():
        for q in range(4):
            outgoing[0:2, q] = packed(2, 4, q)

    first_step = outer

    @pl.when(c == 1)
    def _():
        send_far(first_step)
        send_far(1 - first_step)

    @pl.when(c == 1)
    def _():
        pack_near()

    @pl.when(c == 1)
    def _():
        pl.semaphore_wait(ready, 1)

    def send_near(s):
        remote(outgoing.at[s - 2], arrived.at[s], send_disp.at[1], recv_disp.at[s], toggled(e, s), partner).start()

    @pl.when(c == 1)
    def _():

        @pl.when(outer == 0)
        def _():
            send_near(3)
            send_near(2)

    @pl.when(c == 0)
    def _():
        remote(outgoing.at[0], arrived.at[1], send_disp.at[0], recv_disp.at[1], toggled(e, 1), t).start()

    def down_part(begin, size):
        return remote(
            down_other.at[pl.ds(begin, size)], owned(down_rows, x, c).at[pl.ds(begin, size)], send_weight.at[0], recv_weight.at[0], e, across)

    cut = width // 2 // 16 * 16
    late = c == 1
    fetches[0].wait()
    down_part(0, cut).start()

    @pl.when(jnp.logical_not(late))
    def _():
        down_part(cut, width - cut).start()

    shares = [
        remote(owned(gate_up, 0, c), owned(gate_up, 0, c), send_weight.at[1], recv_weight.at[1], e, partner),
        remote(owned(gate_up, 1, c), owned(gate_up, 1, c), send_weight.at[2], recv_weight.at[2], e, partner),
        remote(owned(down_rows, x, c), owned(down_rows, x, c), send_weight.at[3], recv_weight.at[3], e, partner),
    ]
    for fetch, share in zip(fetches[1:], shares):
        fetch.wait()
        share.start()
    far_rows = owned(down_rows, 1 - x, c)
    relay = remote(far_rows, far_rows, send_weight.at[4], recv_weight.at[4], e, partner)

    logit0, logit1 = logits_ref[0:1, :], logits_ref[1:2, :]
    top = jnp.maximum(logit0, logit1)
    exp0, exp1 = jnp.exp(logit0 - top), jnp.exp(logit1 - top)
    share = prob_ref[...] / (exp0 + exp1)
    weight = jnp.where(at0, share * exp0, 0.0) + jnp.where(at1, share * exp1, 0.0)
    for part in range(2):
        turned = weight[part * (slots // 2):(part + 1) * (slots // 2)].T
        high = turned.astype(BF16)
        weigh[part, 0] = high
        weigh[part, 1] = (turned - high.astype(F32)).astype(BF16)

    def product(left, right):
        return lax.dot_general(left, right, (((1,), (1,)), ((), ())), preferred_element_type=F32)

    def take(s, on=True):
        for q in range(2):
            mine = arrived.at[s, 2 * x + q]
            landed(mine, recv_disp.at[near * q + s])

            @pl.when(on)
            def _():
                remote(mine, mine, send_side.at[0], recv_side.at[s], e, across).start()

    def expand(s, begin=0, wait=None):
        gate = jnp.zeros((capacity, 2 * width), F32)
        up = jnp.zeros((capacity, 2 * width), F32)
        for side in (begin, 1 - begin):
            if wait is not None and side is not begin:
                wait()
            for q in range(2):
                part = arrived[s, 2 * side + q]
                lanes = pl.ds(pl.multiple_of(side * half + q * quarter, quarter), quarter)
                gate = gate + product(part, gate_up[0, :, lanes])
                up = up + product(part, gate_up[1, :, lanes])
        hidden[s, x] = (gate / (1.0 + jnp.exp(-gate)) * up).astype(BF16)
        remote(hidden.at[s, x], hidden.at[s, x], send_hid.at[0], recv_hid.at[s], e, across).start()

    def contract(s):
        acc = jnp.dot(hidden[s, x], down_rows[x], preferred_element_type=F32)
        landed(hidden.at[s, 1 - x], recv_hid.at[s])
        acc = acc + jnp.dot(hidden[s, 1 - x], down_rows[1 - x], preferred_element_type=F32)
        for j in range(2):
            result[s, j] = acc[:, j * quarter:(j + 1) * quarter].astype(BF16)

    def home(s, r, peer, group):
        for j in range(2):
            remote(result.at[s, j], returned.at[r], send_home.at[0], recv_home.at[group], peer, 2 * x + j).start()

    def weights_ready():
        for kind in range(2):
            landed(owned(gate_up, kind, 1 - c), recv_weight.at[1 + kind])

    def relay_down():
        landed(far_rows, recv_weight.at[0])
        relay.start()

    def down_ready():
        landed(owned(down_rows, x, 1 - c), recv_weight.at[3])
        landed(owned(down_rows, 1 - x, 1 - c), recv_weight.at[4])

    def merge(part):
        back = returned[part * near:(part + 1) * near].reshape(slots // 2, quarter)
        return (jnp.dot(weigh[part, 0], back, preferred_element_type=F32)
                + jnp.dot(weigh[part, 1], back, preferred_element_type=F32))

    @pl.when(c == 1)
    def _():
        order = [
            (2 * step + odd, step, odd)
            for step, odd in ((outer, 0), (outer, 1), (1 - outer, 0), (1 - outer, 1))]

        def far_take(i):
            s, step, odd = order[i]
            take(s)

        def far_expand(i):
            s = order[i][0]
            expand(s, x, lambda: landed(arrived.at[s, their_half], recv_side.at[s]))

        def far_contract(i):
            s, step, odd = order[i]
            contract(s)
            home(s, near + s, far_peer(step, odd), 2)

        far_take(0)
        far_take(1)

        @pl.when(outer == 1)
        def _():
            send_near(3)
            send_near(2)


        @pl.when(late)
        def _():
            down_part(cut, width - cut).start()

        weights_ready()
        far_expand(0)
        far_take(2)
        far_expand(1)
        far_take(3)
        relay_down()
        down_ready()
        far_contract(0)
        far_expand(2)
        far_contract(1)
        far_expand(3)
        far_contract(2)
        far_contract(3)
        landed(returned.at[0], recv_home.at[0])

    @pl.when(c == 0)
    def _():
        def near_expand(s):
            if s:
                landed(arrived.at[s], recv_disp.at[s])
            expand(s)

        def near_contract(s):
            contract(s)
            if s:
                home(s, s, toggled(e, s), 1)
            else:
                returned[0] = result[0, 0]
                remote(result.at[0, 1], returned.at[0], send_home.at[0], recv_home.at[0], e, partner).start()

        weights_ready()
        near_expand(0)
        relay_down()
        near_expand(1)
        near_expand(3)
        near_expand(2)
        down_ready()
        near_contract(0)
        near_contract(1)
        near_contract(3)
        near_contract(2)

    landed(returned.at[pl.ds(1, near - 1)], recv_home.at[1])
    total = merge(0)
    landed(returned.at[pl.ds(near, near)], recv_home.at[2])
    out_ref[...] = (total + merge(1)).astype(BF16)

    def finish():
        landed(hidden.at[:, x], send_hid.at[0])
        landed(down_other, send_weight.at[0])
        for share in shares:
            share.wait_send()
        relay.wait_send()

        @pl.when(c == 1)
        def _():
            landed(leaving, send_disp.at[0])
            landed(outgoing, send_disp.at[1])

            landed(arrived.at[:, own_half], send_side.at[0])
            landed(result, send_home.at[0])

        @pl.when(c == 0)
        def _():
            landed(outgoing.at[0], send_disp.at[0])
            landed(returned.at[pl.ds(0, 2 * near - 1)], send_home.at[0])

    finish()


def fused_body(tokens, norm_gain, routes, group_prob, expert_logits, gate_weight, up_weight, down_matrix):
    n_ep = lax.axis_size("ep")
    rows, model = tokens.shape
    capacity = 3 * routes.shape[1] * rows // (2 * n_ep)
    width = gate_weight.shape[2]
    half, quarter = model // 2, model // 4
    sem = pltpu.SemaphoreType.DMA
    vmem = pl.BlockSpec(memory_space=pltpu.VMEM)
    operands = (
        tokens, norm_gain.reshape(1, model), routes.T, group_prob.reshape(1, rows), expert_logits.T,
        gate_weight.reshape(model, width).T, up_weight.reshape(model, width).T, down_matrix.reshape(width, model),
    )
    return pl.pallas_call(
        functools.partial(expert_kernel, n_ep, capacity, width),
        out_shape=jax.ShapeDtypeStruct((rows, quarter), BF16),
        in_specs=[pl.BlockSpec(memory_space=pl.ANY)] * 8,
        out_specs=vmem,
        scratch_shapes=[
            pltpu.VMEM((rows, model), BF16),
            pltpu.VMEM((1, model), F32),
            pltpu.VMEM((2, rows), jnp.int32),
            pltpu.VMEM((1, rows), F32),
            pltpu.VMEM((2, rows), F32),
            pltpu.VMEM((rows, model), BF16),
            pltpu.VMEM((n_ep * capacity, rows), BF16),
            pltpu.VMEM((2, 2, rows, n_ep * capacity // 2), BF16),
            pltpu.VMEM((n_ep // 2, 2, capacity, quarter), BF16),
            pltpu.VMEM((2, capacity, quarter), BF16),
            pltpu.VMEM((2, 4, capacity, quarter), BF16),
            pltpu.VMEM((n_ep // 2, 4, capacity, quarter), BF16),
            pltpu.VMEM((2, 2 * width, model), BF16),
            pltpu.VMEM((2, 2 * width, half), BF16),
            pltpu.VMEM((width, half), BF16),
            pltpu.VMEM((n_ep // 2, 2, capacity, 2 * width), BF16),
            pltpu.VMEM((n_ep // 2, 2, capacity, quarter), BF16),
            pltpu.VMEM((n_ep, capacity, quarter), BF16),
            sem((9,)),
            sem((2,)), sem((n_ep,)),
            sem((1,)), sem((n_ep // 2,)),
            sem((1,)), sem((n_ep // 2,)),
            sem((1,)), sem((3,)),
            sem((5,)), sem((5,)), pltpu.SemaphoreType.REGULAR,
        ],
        compiler_params=pltpu.CompilerParams(
            collective_id=0, has_side_effects=True, vmem_limit_bytes=32 * 1024 * 1024),
    )(*[pltpu.with_memory_space_constraint(operand, pltpu.HBM) for operand in operands])


def fits_kernel(n_ep, n_tp, rows, experts, top, model, width):
    capacity = 3 * top * rows // (2 * experts)
    return (
        experts == n_ep and top == 2 and n_ep == 8 and n_tp == 4
        and capacity % 16 == 0 and rows % 128 == 0 and model % 512 == 0 and width % 16 == 0
    )


def solution(mesh):
    n_ep, n_tp = mesh.shape["ep"], mesh.shape["tp"]

    def chosen(*arrays):
        rows, model = arrays[0].shape
        fits = fits_kernel(n_ep, n_tp, rows, arrays[5].shape[0] * n_ep, arrays[2].shape[1], model, arrays[5].shape[2])
        return (fused_body if fits else body)(*arrays)

    return jax.shard_map(
        chosen,
        mesh=mesh,
        in_specs=(
            P("ep", None),
            P(),
            P("ep", None),
            P("ep"),
            P("ep", None),
            P("ep", None, "tp"),
            P("ep", None, "tp"),
            P("ep", "tp", None),
        ),
        out_specs=P("ep", "tp"),
        check_vma=False,
    )
```

```python
import functools

import jax
import jax.numpy as jnp
from jax import lax
from jax.experimental import pallas as pl
from jax.experimental.pallas import tpu as pltpu
from jax.sharding import PartitionSpec as P


def hidden_part(buffer, gate_weight, up_weight):
    local_count = gate_weight.shape[0]
    grouped = buffer.reshape(
        buffer.shape[0] // local_count, local_count, buffer.shape[1], buffer.shape[2]
    )
    gate_proj = jnp.einsum(
        "sknd,kdf->sknf", grouped, gate_weight, preferred_element_type=jnp.float32
    )
    up_proj = jnp.einsum("sknd,kdf->sknf", grouped, up_weight, preferred_element_type=jnp.float32)
    hidden_state = (jax.nn.silu(gate_proj) * up_proj).astype(jnp.bfloat16)
    return hidden_state.reshape(buffer.shape[0], buffer.shape[1], hidden_state.shape[3])


def down_blocks(hidden_full, down_cols, block_count):
    local_count = down_cols.shape[0]
    width = hidden_full.shape[2] // block_count
    grouped = hidden_full.reshape(
        hidden_full.shape[0] // local_count, local_count, hidden_full.shape[1], block_count, width
    )
    columns = down_cols.reshape(local_count, block_count, width, down_cols.shape[2])
    block_list = jnp.einsum(
        "sknrf,krfd->sknrd", grouped, columns, preferred_element_type=jnp.float32
    ).astype(jnp.bfloat16)
    summed = jnp.sum(block_list.astype(jnp.float32), 3).astype(jnp.bfloat16)
    return summed.reshape(hidden_full.shape[0], hidden_full.shape[1], down_cols.shape[2])


def body(tokens, norm_gain, routes, group_prob, expert_logits, gate_weight, up_weight, down_matrix):
    tok_rows, model_width = tokens.shape
    top_count = routes.shape[1]
    experts = gate_weight.shape[0] * lax.axis_size("ep")
    capacity = 3 * top_count * tok_rows // (2 * experts)
    block_count = lax.axis_size("tp")
    down_cols = lax.all_to_all(down_matrix, "tp", split_axis=2, concat_axis=1, tiled=True)
    values = tokens.astype(jnp.float32)
    normed = (
        values * lax.rsqrt(jnp.mean(values * values, -1, keepdims=True) + 1e-06) * norm_gain
    ).astype(jnp.bfloat16)
    flat_ids = routes.reshape(-1)
    onehot = (flat_ids[:, None] == jnp.arange(experts, dtype=jnp.int32)[None, :]).astype(jnp.int32)
    earlier = jnp.cumsum(onehot, 0) - onehot
    slot_index = jnp.sum(earlier * onehot, 1)
    target = flat_ids * capacity + slot_index
    owners = jnp.arange(tok_rows * top_count, dtype=jnp.int32) // top_count
    outgoing = (
        jnp.zeros((experts * capacity, model_width), jnp.bfloat16).at[target].set(normed[owners])
    )
    outgoing = outgoing.reshape(experts, capacity, model_width)
    hidden_state = hidden_part(
        lax.all_to_all(outgoing, "ep", split_axis=0, concat_axis=0, tiled=True),
        gate_weight,
        up_weight,
    )
    hidden_full = lax.all_gather(hidden_state, "tp", axis=2, tiled=True)
    summed = down_blocks(hidden_full, down_cols, block_count)
    returned = lax.all_to_all(summed, "ep", split_axis=0, concat_axis=0, tiled=True)
    flat_back = returned.reshape(experts * capacity, returned.shape[2])
    weights = group_prob[:, None] * jax.nn.softmax(expert_logits, axis=-1)
    picked = flat_back[target].reshape(tok_rows, top_count, flat_back.shape[1]).astype(jnp.float32)
    combined = jnp.sum(picked * weights[:, :, None], 1).astype(jnp.bfloat16)
    return combined


MESH = pl.DeviceIdType.MESH
F32, BF16 = jnp.float32, jnp.bfloat16


def round_up(value, step):
    return -(-value // step) * step


def flipped(index, bit):
    return bit * (1 - 2 * ((index // bit) % 2))


def toggled(index, mask):
    result, bit = index, 1
    while bit <= mask:
        if mask & bit:
            result = result + flipped(index, bit)
        bit *= 2
    return result


def expert_kernel(
    n_ep, capacity, width,
    tokens_hbm, gain_hbm, routes_hbm, prob_hbm, logits_hbm, gate_ref, up_ref, down_ref,
    out_ref,
    tokens_ref, gain_ref, routes_ref, prob_ref, logits_ref, normed, select, weigh, leaving, spare, outgoing, arrived, gate_up,
    down_rows, down_other, hidden, result, returned,
    load_sem, send_disp, recv_disp, send_side, recv_side, send_hid, recv_hid, send_home, recv_home, send_weight, recv_weight, ready,
):
    loads = [
        pltpu.make_async_copy(source, target, load_sem.at[i])
        for i, (source, target) in enumerate((
            (routes_hbm, routes_ref), (tokens_hbm, tokens_ref), (gain_hbm, gain_ref),
            (prob_hbm, prob_ref), (logits_hbm, logits_ref),
        ))
    ]
    for load in loads:
        load.start()
    rows, model = tokens_ref.shape
    half, quarter = model // 2, model // 4
    near = n_ep // 2
    slots = n_ep * capacity
    e = lax.axis_index("ep")
    t = lax.axis_index("tp")
    x, c = t // 2, t % 2
    partner, across = t + 1 - 2 * c, (t + 2) % 4
    outer = 1 - ((e // 2) % 2 + (e // 4) % 2) % 2

    hi, lo = e // 4, (e // 2) % 2

    barrier = pltpu.get_barrier_semaphore()

    def greet(semaphore, ep, tp):
        pl.semaphore_signal(semaphore, inc=1, device_id={"ep": ep, "tp": tp}, device_id_type=MESH)

    for r in reversed(range(1, n_ep)):
        greet(barrier, toggled(e, r), t)
    greet(barrier, e, across)

    @pl.when(c == 1)
    def _():
        for r in reversed(range(n_ep)):
            greet(barrier, toggled(e, r), partner)

    def columns(side):
        return pl.ds(pl.multiple_of(side * half, half), half)

    def owned(ref, side, core):
        return ref.at[side, pl.ds(pl.multiple_of(core * width, width), width)]

    def both(ref, core):
        return ref.at[:, pl.ds(pl.multiple_of(core * width, width), width)]

    fetches = [
        pltpu.make_async_copy(down_ref.at[:, columns(1 - x)], down_other, load_sem.at[5]),
        pltpu.make_async_copy(gate_ref, owned(gate_up, 0, c), load_sem.at[6]),
        pltpu.make_async_copy(up_ref, owned(gate_up, 1, c), load_sem.at[7]),
        pltpu.make_async_copy(down_ref.at[:, columns(x)], owned(down_rows, x, c), load_sem.at[8]),
    ]
    for fetch in fetches:
        fetch.start()
    for load in loads:
        load.wait()

    first, second = routes_ref[0:1, :], routes_ref[1:2, :]
    lanes = round_up(n_ep, 16)
    expert_row = lax.broadcasted_iota(jnp.int32, (lanes, rows), 0)
    hit0 = (expert_row == first).astype(F32)
    hit1 = (expert_row == second).astype(F32)
    before = (
        lax.broadcasted_iota(jnp.int32, (rows, rows), 0) < lax.broadcasted_iota(jnp.int32, (rows, rows), 1)
    ).astype(F32).astype(BF16)
    earlier = jnp.dot((hit0 + hit1).astype(BF16), before, preferred_element_type=F32)
    slot0 = jnp.sum(earlier * hit0, 0, keepdims=True)
    slot1 = jnp.sum(earlier * hit1, 0, keepdims=True)
    place0 = (first ^ e) * capacity + slot0.astype(jnp.int32)
    place1 = (second ^ e) * capacity + slot1.astype(jnp.int32)
    slot_row = lax.broadcasted_iota(jnp.int32, (slots, rows), 0)
    at0, at1 = slot_row == place0, slot_row == place1
    select[...] = (at0.astype(F32) + at1.astype(F32)).astype(BF16)

    values = tokens_ref[...].astype(F32)
    scale = lax.rsqrt(jnp.mean(values * values, -1, keepdims=True) + 1e-06)
    normed[...] = (values * scale * gain_ref[...]).astype(BF16)

    def packed(begin, end, q):
        lanes = pl.ds(pl.multiple_of(q * quarter, quarter), quarter)
        return jnp.dot(
            select[begin * capacity:end * capacity], normed[:, lanes], preferred_element_type=F32
        ).astype(BF16).reshape(end - begin, capacity, quarter)

    @pl.when(c == 1)
    def _():
        for q in range(2):
            leaving[:, q] = packed(near, n_ep, 2 * x + q)

    @pl.when(c == 0)
    def _():
        for q in range(4):
            both = packed(0, 2, q)
            arrived[0, q] = both[0]
            outgoing[0, q] = both[1]

    @pl.when(c == 1)
    def _():
        pl.semaphore_wait(barrier, n_ep)

    @pl.when(c == 0)
    def _():
        pl.semaphore_wait(barrier, 2 * n_ep)
        greet(ready, e, partner)

    def remote(source, target, send, recv, ep, tp):
        return pltpu.make_async_remote_copy(
            src_ref=source, dst_ref=target, send_sem=send, recv_sem=recv,
            device_id={"ep": ep, "tp": tp}, device_id_type=MESH)

    def landed(ref, sem):
        pltpu.make_async_copy(ref, ref, sem).wait()

    own_half, their_half = pl.ds(2 * x, 2), pl.ds(2 - 2 * x, 2)

    def far_peer(step, odd):
        return e + flipped(e, 4) + step * flipped(e, 2) + odd * flipped(e, 1)

    def send_far(step):
        for odd in range(2):
            s = 2 * step + odd
            for q in range(2):
                remote(
                    leaving.at[s, q], arrived.at[s, 2 * x + q], send_disp.at[0], recv_disp.at[near * q + s],
                    far_peer(step, odd), t).start()

    def pack_near():
        for q in range(4):
            outgoing[0:2, q] = packed(2, 4, q)

    first_step = outer

    @pl.when(c == 1)
    def _():
        send_far(first_step)
        send_far(1 - first_step)

    @pl.when(c == 1)
    def _():
        pack_near()

    @pl.when(c == 1)
    def _():
        pl.semaphore_wait(ready, 1)

    def send_near(s):
        remote(outgoing.at[s - 2], arrived.at[s], send_disp.at[1], recv_disp.at[s], toggled(e, s), partner).start()

    @pl.when(c == 1)
    def _():

        @pl.when(outer == 0)
        def _():
            send_near(3)
            send_near(2)

    @pl.when(c == 0)
    def _():
        remote(outgoing.at[0], arrived.at[1], send_disp.at[0], recv_disp.at[1], toggled(e, 1), t).start()

    def down_part(begin, size):
        return remote(
            down_other.at[pl.ds(begin, size)], owned(down_rows, x, c).at[pl.ds(begin, size)], send_weight.at[0], recv_weight.at[0], e, across)

    cut = width // 2 // 16 * 16
    late = c == 1
    fetches[0].wait()
    down_part(0, cut).start()

    @pl.when(jnp.logical_not(late))
    def _():
        down_part(cut, width - cut).start()

    shares = [
        remote(owned(gate_up, 0, c), owned(gate_up, 0, c), send_weight.at[1], recv_weight.at[1], e, partner),
        remote(owned(gate_up, 1, c), owned(gate_up, 1, c), send_weight.at[1], recv_weight.at[1], e, partner),
        remote(owned(down_rows, x, c), owned(down_rows, x, c), send_weight.at[0], recv_weight.at[2], e, partner),
    ]
    for fetch, share in zip(fetches[1:], shares):
        fetch.wait()
        share.start()
    far_rows = owned(down_rows, 1 - x, c)
    relay = remote(far_rows, far_rows, send_weight.at[0], recv_weight.at[2], e, partner)

    logit0, logit1 = logits_ref[0:1, :], logits_ref[1:2, :]
    top = jnp.maximum(logit0, logit1)
    exp0, exp1 = jnp.exp(logit0 - top), jnp.exp(logit1 - top)
    share = prob_ref[...] / (exp0 + exp1)
    weight = jnp.where(at0, share * exp0, 0.0) + jnp.where(at1, share * exp1, 0.0)
    for part in range(2):
        turned = weight[part * (slots // 2):(part + 1) * (slots // 2)].T
        high = turned.astype(BF16)
        weigh[part, 0] = high
        weigh[part, 1] = (turned - high.astype(F32)).astype(BF16)

    def product(left, right):
        return lax.dot_general(left, right, (((1,), (1,)), ((), ())), preferred_element_type=F32)

    def take(s, on=True):
        for q in range(2):
            mine = arrived.at[s, 2 * x + q]
            landed(mine, recv_disp.at[near * q + s])

            @pl.when(on)
            def _():
                remote(mine, mine, send_side.at[0], recv_side.at[s], e, across).start()

    def expand(s, begin=0, wait=None):
        gate = jnp.zeros((capacity, 2 * width), F32)
        up = jnp.zeros((capacity, 2 * width), F32)
        for side in (begin, 1 - begin):
            if wait is not None and side is not begin:
                wait()
            for q in range(2):
                part = arrived[s, 2 * side + q]
                lanes = pl.ds(pl.multiple_of(side * half + q * quarter, quarter), quarter)
                gate = gate + product(part, gate_up[0, :, lanes])
                up = up + product(part, gate_up[1, :, lanes])
        hidden[s, x] = (gate / (1.0 + jnp.exp(-gate)) * up).astype(BF16)
        remote(hidden.at[s, x], hidden.at[s, x], send_hid.at[0], recv_hid.at[s], e, across).start()

    def contract(s):
        acc = jnp.dot(hidden[s, x], down_rows[x], preferred_element_type=F32)
        landed(hidden.at[s, 1 - x], recv_hid.at[s])
        acc = acc + jnp.dot(hidden[s, 1 - x], down_rows[1 - x], preferred_element_type=F32)
        for j in range(2):
            result[s, j] = acc[:, j * quarter:(j + 1) * quarter].astype(BF16)

    def home(s, r, peer, group):
        for j in range(2):
            remote(result.at[s, j], returned.at[r], send_home.at[0], recv_home.at[group], peer, 2 * x + j).start()

    def weights_ready():
        landed(both(gate_up, 1 - c), recv_weight.at[1])

    def relay_down():
        landed(far_rows, recv_weight.at[0])
        relay.start()

    def down_ready():
        landed(both(down_rows, 1 - c), recv_weight.at[2])

    def merge(part):
        back = returned[part * near:(part + 1) * near].reshape(slots // 2, quarter)
        return (jnp.dot(weigh[part, 0], back, preferred_element_type=F32)
                + jnp.dot(weigh[part, 1], back, preferred_element_type=F32))

    @pl.when(c == 1)
    def _():
        order = [
            (2 * step + odd, step, odd)
            for step, odd in ((outer, 0), (outer, 1), (1 - outer, 0), (1 - outer, 1))]

        def far_take(i):
            s, step, odd = order[i]
            take(s)

        def far_expand(i):
            s = order[i][0]
            expand(s, x, lambda: landed(arrived.at[s, their_half], recv_side.at[s]))

        def far_contract(i):
            s, step, odd = order[i]
            contract(s)
            home(s, near + s, far_peer(step, odd), 2)

        far_take(0)
        far_take(1)

        @pl.when(outer == 1)
        def _():
            send_near(3)
            send_near(2)


        @pl.when(late)
        def _():
            down_part(cut, width - cut).start()

        weights_ready()
        far_expand(0)
        far_take(2)
        far_expand(1)
        far_take(3)
        relay_down()
        down_ready()
        far_contract(0)
        far_expand(2)
        far_contract(1)
        far_expand(3)
        far_contract(2)
        far_contract(3)
        landed(returned.at[0], recv_home.at[0])

    @pl.when(c == 0)
    def _():
        def near_expand(s):
            if s:
                landed(arrived.at[s], recv_disp.at[s])
            expand(s)

        def near_contract(s):
            contract(s)
            if s:
                home(s, s, toggled(e, s), 1)
            else:
                returned[0] = result[0, 0]
                remote(result.at[0, 1], returned.at[0], send_home.at[0], recv_home.at[0], e, partner).start()

        weights_ready()
        near_expand(0)
        relay_down()
        near_expand(1)
        near_expand(3)
        near_expand(2)
        down_ready()
        near_contract(0)
        near_contract(1)
        near_contract(3)
        near_contract(2)

    landed(returned.at[pl.ds(1, near - 1)], recv_home.at[1])
    total = merge(0)
    landed(returned.at[pl.ds(near, near)], recv_home.at[2])
    out_ref[...] = (total + merge(1)).astype(BF16)

    def finish():
        landed(hidden.at[:, x], send_hid.at[0])
        landed(down_rows.at[:, pl.ds(0, 3 * width // 2)], send_weight.at[0])
        landed(both(gate_up, c), send_weight.at[1])

        @pl.when(c == 1)
        def _():
            landed(leaving, send_disp.at[0])
            landed(outgoing, send_disp.at[1])

            landed(arrived.at[:, own_half], send_side.at[0])
            landed(result, send_home.at[0])

        @pl.when(c == 0)
        def _():
            landed(outgoing.at[0], send_disp.at[0])
            landed(returned.at[pl.ds(0, 2 * near - 1)], send_home.at[0])

    finish()


def fused_body(tokens, norm_gain, routes, group_prob, expert_logits, gate_weight, up_weight, down_matrix):
    n_ep = lax.axis_size("ep")
    rows, model = tokens.shape
    capacity = 3 * routes.shape[1] * rows // (2 * n_ep)
    width = gate_weight.shape[2]
    half, quarter = model // 2, model // 4
    sem = pltpu.SemaphoreType.DMA
    vmem = pl.BlockSpec(memory_space=pltpu.VMEM)
    operands = (
        tokens, norm_gain.reshape(1, model), routes.T, group_prob.reshape(1, rows), expert_logits.T,
        gate_weight.reshape(model, width).T, up_weight.reshape(model, width).T, down_matrix.reshape(width, model),
    )
    return pl.pallas_call(
        functools.partial(expert_kernel, n_ep, capacity, width),
        out_shape=jax.ShapeDtypeStruct((rows, quarter), BF16),
        in_specs=[pl.BlockSpec(memory_space=pl.ANY)] * 8,
        out_specs=vmem,
        scratch_shapes=[
            pltpu.VMEM((rows, model), BF16),
            pltpu.VMEM((1, model), F32),
            pltpu.VMEM((2, rows), jnp.int32),
            pltpu.VMEM((1, rows), F32),
            pltpu.VMEM((2, rows), F32),
            pltpu.VMEM((rows, model), BF16),
            pltpu.VMEM((n_ep * capacity, rows), BF16),
            pltpu.VMEM((2, 2, rows, n_ep * capacity // 2), BF16),
            pltpu.VMEM((n_ep // 2, 2, capacity, quarter), BF16),
            pltpu.VMEM((2, capacity, quarter), BF16),
            pltpu.VMEM((2, 4, capacity, quarter), BF16),
            pltpu.VMEM((n_ep // 2, 4, capacity, quarter), BF16),
            pltpu.VMEM((2, 2 * width, model), BF16),
            pltpu.VMEM((2, 2 * width, half), BF16),
            pltpu.VMEM((width, half), BF16),
            pltpu.VMEM((n_ep // 2, 2, capacity, 2 * width), BF16),
            pltpu.VMEM((n_ep // 2, 2, capacity, quarter), BF16),
            pltpu.VMEM((n_ep, capacity, quarter), BF16),
            sem((9,)),
            sem((2,)), sem((n_ep,)),
            sem((1,)), sem((n_ep // 2,)),
            sem((1,)), sem((n_ep // 2,)),
            sem((1,)), sem((3,)),
            sem((2,)), sem((3,)), pltpu.SemaphoreType.REGULAR,
        ],
        compiler_params=pltpu.CompilerParams(
            collective_id=0, has_side_effects=True, vmem_limit_bytes=32 * 1024 * 1024),
    )(*[pltpu.with_memory_space_constraint(operand, pltpu.HBM) for operand in operands])


def fits_kernel(n_ep, n_tp, rows, experts, top, model, width):
    capacity = 3 * top * rows // (2 * experts)
    return (
        experts == n_ep and top == 2 and n_ep == 8 and n_tp == 4
        and capacity % 16 == 0 and rows % 128 == 0 and model % 512 == 0 and width % 32 == 0
    )


def solution(mesh):
    n_ep, n_tp = mesh.shape["ep"], mesh.shape["tp"]

    def chosen(*arrays):
        rows, model = arrays[0].shape
        fits = fits_kernel(n_ep, n_tp, rows, arrays[5].shape[0] * n_ep, arrays[2].shape[1], model, arrays[5].shape[2])
        return (fused_body if fits else body)(*arrays)

    return jax.shard_map(
        chosen,
        mesh=mesh,
        in_specs=(
            P("ep", None),
            P(),
            P("ep", None),
            P("ep"),
            P("ep", None),
            P("ep", None, "tp"),
            P("ep", None, "tp"),
            P("ep", "tp", None),
        ),
        out_specs=P("ep", "tp"),
        check_vma=False,
    )
```
